32 devices in a mesh: sp: 4 (over y, x), tp: 8 (over z, core).
Axes of the slice: x: 2, y: 2, z: 4, core: 2. Of those that a mesh axis runs over, the one named last changes fastest.
Arguments:
- residual: bfloat16 [4096, 2048], P(('sp', 'tp')), may hold values from -6 to 6
- wide_query: bfloat16 [4096, 1024], P('sp', 'tp'), may hold values from -8 to 8
- narrow_query: bfloat16 [4096, 1024], P('sp', 'tp'), may hold values from -8 to 8
- wide_keys: bfloat16 [4096, 256], P('sp'), may hold values from -6 to 6
- narrow_keys: bfloat16 [4096, 256], P('sp'), may hold values from -6 to 6
- wide_values: bfloat16 [4096, 256], P('sp'), may hold values from -6 to 6
- narrow_values: bfloat16 [4096, 256], P('sp'), may hold values from -6 to 6
- wide_query_gain: float32 [64], replicated, may hold values from 1.2 to 10
- wide_key_gain: float32 [64], replicated, may hold values from 1.2 to 10
- narrow_query_gain: float32 [32], replicated, may hold values from 1.2 to 10
- narrow_key_gain: float32 [32], replicated, may hold values from 1.2 to 10
- wide_out: bfloat16 [1024, 2048], P('tp'), may hold values from -0.25 to 0.25
- narrow_out: bfloat16 [1024, 2048], P('tp'), may hold values from -0.25 to 0.25
- first_gain: float32 [2048], replicated, may hold values from 0.1 to 1.9
- first_bias: float32 [2048], replicated, may hold values from -1.8 to 1.8
- route_ids: int32 [4096, 2], P(('sp', 'tp')), may hold values from 0 to 7, all different within a row; in each aligned block of 128 rows (0 to 127, 128 to 255, ...) at most 40 rows name the same one
- route_weights: float32 [4096, 2], P(('sp', 'tp')), may hold values from 0.25 to 2.5
- expert_gate: bfloat16 [8, 2048, 3072], P('sp', None, 'tp'), may hold values from -0.125 to 0.125
- expert_up: bfloat16 [8, 2048, 3072], P('sp', None, 'tp'), may hold values from -0.125 to 0.125
- expert_down: bfloat16 [8, 3072, 2048], P('sp', 'tp'), may hold values from -0.109375 to 0.109375
- shared_gate: bfloat16 [2048, 256], replicated, may hold values from -0.125 to 0.125
- shared_up: bfloat16 [2048, 256], replicated, may hold values from -0.125 to 0.125
- shared_down: bfloat16 [256, 2048], replicated, may hold values from -0.375 to 0.375
- second_gain: float32 [2048], replicated, may hold values from 0.1 to 1.9
- second_bias: float32 [2048], replicated, may hold values from -1.8 to 1.8
Outputs:
- layer_output: bfloat16 [4096, 2048], P(('sp', 'tp'))
The draws below stay inside these ranges and needn't reach their ends.
Inputs may be any that keep to these rules, and one draw needn't show every extreme that they name: `route_ids`: each row names 2 different experts. The rows of one device (aligned blocks of 128 rows) name each expert at most 40 times, and in every draw some expert is named exactly 40 times in the rows of some device.
All inputs are finite; a program needn't handle non-finite values.
Results may differ from the reference program's by a relative error of at most 0.02.
The reference program's roundings to bfloat16 on the way count: a program that leaves them out, or rounds other values in their place, can miss the bound.
Values may be sent and summed in bfloat16 or wider, within the bound.
A program may use at most 128 MiB of HBM per device.

```python
import math
import jax
import jax.numpy as jnp
import numpy as np
from jax import lax

MODEL_WIDTH = 2048
WIDE_HEADS = 16
WIDE_SIZE = 64
WIDE_GROUPS = 4
NARROW_HEADS = 32
NARROW_SIZE = 32
NARROW_GROUPS = 8
GRID_WIDTH = 64
EXPERT_WIDTH = 3072
SHARED_WIDTH = 256
ROUTE_TOP = 2
SEQ_TOKENS = 4096
TOKENS = 4096
DEVICE_ROWS = 128
EXPERTS = 8
CAPACITY = 40
N_SP = 4
N_TP = 8


def gain_pair(key, head_size, salt):
    folded = jax.random.fold_in(key, salt)
    draw_one = jax.random.uniform(jax.random.fold_in(folded, 2), (head_size,), jnp.float32)
    draw_two = jax.random.uniform(jax.random.fold_in(folded, 3), (head_size,), jnp.float32)
    query_gain = 1.5 * 2.0 ** draw_one
    key_gain = 1.5 * 2.0 ** draw_two
    return (query_gain, key_gain)


def field(key, heads, head_size, salt):
    folded = jax.random.fold_in(key, salt)
    return jnp.clip(jax.random.normal(folded, (TOKENS, heads, head_size), jnp.float32), -6.0, 6.0)


def drawn_queries(key, heads, head_size, salt):
    values = field(key, heads, head_size, salt + 100)
    return values.reshape(TOKENS, heads * head_size).astype(jnp.bfloat16)


def drawn_keys(key, heads, head_size, salt):
    values = field(key, heads, head_size, salt + 300)
    return values.reshape(TOKENS, heads * head_size).astype(jnp.bfloat16)


def draw_wide_query(key, part):
    return drawn_queries(key, WIDE_HEADS, WIDE_SIZE, 11)


def draw_narrow_query(key, part):
    return drawn_queries(key, NARROW_HEADS, NARROW_SIZE, 23)


def draw_wide_keys(key, part):
    return drawn_keys(key, WIDE_GROUPS, WIDE_SIZE, 11)


def draw_narrow_keys(key, part):
    return drawn_keys(key, NARROW_GROUPS, NARROW_SIZE, 23)


def draw_wide_query_gain(key, part):
    return gain_pair(key, WIDE_SIZE, 11)[0]


def draw_wide_key_gain(key, part):
    return gain_pair(key, WIDE_SIZE, 11)[1]


def draw_narrow_query_gain(key, part):
    return gain_pair(key, NARROW_SIZE, 23)[0]


def draw_narrow_key_gain(key, part):
    return gain_pair(key, NARROW_SIZE, 23)[1]


def levels(own_key, extent, shards, smallest, top_value):
    factor_of, own = 1.0, jax.random.fold_in(own_key, 6)
    for dim, parts in shards:
        heights = jnp.exp(jax.random.uniform(jax.random.fold_in(own, dim), (parts,), jnp.float32, smallest / len(shards), top_value / len(shards)))
        factor_of = factor_of * jnp.repeat(heights, extent[dim] // parts).reshape([-1 if axis == dim else 1 for axis in range(len(extent))])
    return factor_of


def shared_out(own_key, own, number, rows, number_of, top, bound, slope):
    ranking = jax.random.permutation(own_key, number_of)
    packed, usual = shares(number_of, rows * top, bound, slope, True), shares(number_of, rows * top, bound, slope, False)
    places = jnp.arange(number_of)

    def named(sizes, rotation):
        used = int((sizes > 0).sum())
        fixed = max(1, used // 4)
        passed = fixed + (places - fixed + rotation * (used - fixed)) % max(1, number_of - fixed)
        return jnp.zeros((number_of,), jnp.int32).at[ranking[jnp.where(places < fixed, places, passed)]].set(jnp.asarray(sizes, jnp.int32))

    sizes = jnp.where(number % 4 == 0, named(packed, number // 4), named(usual, number - number // 4 - 1))
    mixed = jax.random.permutation(jax.random.fold_in(own, 3), number_of)
    giver, sink = mixed[0:number_of // 2 * 2:2], mixed[1:number_of // 2 * 2:2]
    room = jnp.minimum(sizes[giver] - 1, bound - sizes[sink]) // 2
    room = jnp.where((giver == ranking[0]) | (sink == ranking[0]) | (sizes[sink] == 0), 0, jnp.maximum(room, 0))
    passed = jax.random.randint(jax.random.fold_in(own, 4), (number_of // 2,), 0, 1 << 20) % (room + 1)
    sizes = sizes.at[giver].add(-passed).at[sink].add(passed)
    items = jnp.searchsorted(jnp.cumsum(sizes), jnp.arange(rows * top), side="right").astype(jnp.int32)
    table = items.reshape(top, rows).T
    table = table[jax.random.permutation(jax.random.fold_in(own, 1), rows)]
    rotation = jax.random.randint(jax.random.fold_in(own, 2), (rows, 1), 0, top)
    return jnp.take_along_axis(table, (jnp.arange(top)[None, :] + rotation) % top, axis=1)


def shares(number_of, total, most, lean, full):
    weights = [(1 << 20) // math.isqrt(rank ** lean) + 1 for rank in range(1, number_of + 1)]
    largest = most if full else min(most, max(-(-total // number_of), total * weights[0] // sum(weights)))
    least = 1 if total - largest >= number_of - 1 else 0
    given, surplus = [largest] + [least] * (number_of - 1), total - largest - least * (number_of - 1)
    while surplus > 0:
        movable = [i for i in range(1, number_of) if given[i] < largest] or [i for i in range(1, number_of) if given[i] < most]
        pool, left = sum([weights[i] for i in movable]), surplus
        for i in movable:
            more = min(most - given[i], max(1, left * weights[i] // pool), surplus)
            given[i] = given[i] + more
            surplus = surplus - more
    return np.array(given)


def gaussian(rng, shape, scale, limit, cuts=(), kind=jnp.bfloat16):
    values = jax.random.normal(rng, shape, jnp.float32) * scale
    if len(cuts) > 0:
        values = levels(rng, shape, cuts, -0.22, 0.18) * values
    return jnp.clip(values, min=-limit, max=limit).astype(kind)


def setup_inputs(seed: int = 0) -> dict:
    streams_of = jax.random.split(jax.random.key(seed), 26)
    residual = gaussian(streams_of[0], (TOKENS, MODEL_WIDTH), 1.0, 6.0, ((0, 32),))
    wide_query = draw_wide_query(jax.random.fold_in(streams_of[25], 71), 0)
    narrow_query = draw_narrow_query(jax.random.fold_in(streams_of[25], 71), 0)
    wide_keys = draw_wide_keys(jax.random.fold_in(streams_of[25], 71), 0)
    narrow_keys = draw_narrow_keys(jax.random.fold_in(streams_of[25], 71), 0)
    wide_values = gaussian(streams_of[5], (TOKENS, WIDE_GROUPS * WIDE_SIZE), 1.0, 6.0, ((0, 4),))
    narrow_values = gaussian(streams_of[6], (TOKENS, NARROW_GROUPS * NARROW_SIZE), 1.0, 6.0, ((0, 4),))
    wide_query_gain = draw_wide_query_gain(jax.random.fold_in(streams_of[25], 71), 0)
    wide_key_gain = draw_wide_key_gain(jax.random.fold_in(streams_of[25], 71), 0)
    narrow_query_gain = draw_narrow_query_gain(jax.random.fold_in(streams_of[25], 71), 0)
    narrow_key_gain = draw_narrow_key_gain(jax.random.fold_in(streams_of[25], 71), 0)
    wide_out = gaussian(streams_of[11], (WIDE_HEADS * WIDE_SIZE, MODEL_WIDTH), (WIDE_HEADS * WIDE_SIZE // 2) ** -0.5, 0.25, ((0, 8),))
    narrow_out = gaussian(streams_of[12], (NARROW_HEADS * NARROW_SIZE, MODEL_WIDTH), (NARROW_HEADS * NARROW_SIZE // 2) ** -0.5, 0.25, ((0, 8),))
    first_gain = jnp.clip(1.0 + 0.18 * jax.random.normal(streams_of[13], (MODEL_WIDTH,), jnp.float32), 0.1, 1.9)
    first_bias = gaussian(streams_of[14], (MODEL_WIDTH,), 0.3, 1.8, (), jnp.float32)
    route_ids_keys = jax.random.split(jax.random.fold_in(streams_of[15], 1), TOKENS // DEVICE_ROWS)
    route_ids_turns = jax.random.permutation(jax.random.fold_in(streams_of[15], 3), TOKENS // DEVICE_ROWS)
    route_ids = jax.vmap(lambda own, number: shared_out(jax.random.fold_in(streams_of[15], 2), own, number, DEVICE_ROWS, EXPERTS, ROUTE_TOP, CAPACITY, 2))(route_ids_keys, route_ids_turns).reshape((TOKENS, ROUTE_TOP))
    route_weights = jnp.clip(jnp.exp(math.log(2.5) - 2.3025851 * jax.random.uniform(streams_of[16], (TOKENS, ROUTE_TOP), jnp.float32) ** levels(streams_of[16], (TOKENS, ROUTE_TOP), ((0, 32),), -0.2, 0.2)), 0.25, 2.5)
    expert_gate = gaussian(streams_of[17], (EXPERTS, MODEL_WIDTH, EXPERT_WIDTH), MODEL_WIDTH ** -0.5, 0.125, ((0, 4), (2, 8)))
    expert_up = gaussian(streams_of[18], (EXPERTS, MODEL_WIDTH, EXPERT_WIDTH), MODEL_WIDTH ** -0.5, 0.125, ((0, 4), (2, 8)))
    expert_down = gaussian(streams_of[19], (EXPERTS, EXPERT_WIDTH, MODEL_WIDTH), EXPERT_WIDTH ** -0.5, 0.109375, ((0, 4), (1, 8)))
    shared_gate = gaussian(streams_of[20], (MODEL_WIDTH, SHARED_WIDTH), MODEL_WIDTH ** -0.5, 0.125)
    shared_up = gaussian(streams_of[21], (MODEL_WIDTH, SHARED_WIDTH), MODEL_WIDTH ** -0.5, 0.125)
    shared_down = gaussian(streams_of[22], (SHARED_WIDTH, MODEL_WIDTH), SHARED_WIDTH ** -0.5, 0.375)
    second_gain = jnp.clip(1.0 + 0.18 * jax.random.normal(streams_of[23], (MODEL_WIDTH,), jnp.float32), 0.1, 1.9)
    second_bias = gaussian(streams_of[24], (MODEL_WIDTH,), 0.3, 1.8, (), jnp.float32)
    return {"residual": residual, "wide_query": wide_query, "narrow_query": narrow_query, "wide_keys": wide_keys, "narrow_keys": narrow_keys, "wide_values": wide_values, "narrow_values": narrow_values, "wide_query_gain": wide_query_gain, "wide_key_gain": wide_key_gain, "narrow_query_gain": narrow_query_gain, "narrow_key_gain": narrow_key_gain, "wide_out": wide_out, "narrow_out": narrow_out, "first_gain": first_gain, "first_bias": first_bias, "route_ids": route_ids, "route_weights": route_weights, "expert_gate": expert_gate, "expert_up": expert_up, "expert_down": expert_down, "shared_gate": shared_gate, "shared_up": shared_up, "shared_down": shared_down, "second_gain": second_gain, "second_bias": second_bias}


EPS_HEAD = 1e-06
EPS_LAYER = 1e-05
ALPHA = 2.0 ** 0.25
THETA = 10000.0

def head_norm(values, gain_vec):
    mean_square = lax.optimization_barrier(jnp.mean(values * values, axis=-1, keepdims=True))
    return values * lax.rsqrt(mean_square + EPS_HEAD) * gain_vec

def rotate(values, position):
    half_size = values.shape[-1] // 2
    frequency = THETA ** (-jnp.arange(half_size, dtype=jnp.float32) / half_size)
    angles = position.astype(jnp.float32)[:, None] * frequency
    cosine = jnp.cos(angles)[:, None, :]
    sine_part = jnp.sin(angles)[:, None, :]
    leading = values[..., :half_size]
    trailing = values[..., half_size:]
    return jnp.concatenate([leading * cosine - trailing * sine_part, trailing * cosine + leading * sine_part], axis=-1)

def grid_rotate(values, position):
    half_size = values.shape[-1] // 2
    grid_row = position // GRID_WIDTH
    grid_col = position % GRID_WIDTH
    return jnp.concatenate([rotate(values[..., :half_size], grid_row), rotate(values[..., half_size:], grid_col)], axis=-1)

def layer_norm(values, gain_vec, bias_vec):
    center = lax.optimization_barrier(jnp.mean(values, axis=-1, keepdims=True))
    shifted = values - center
    variance = lax.optimization_barrier(jnp.mean(shifted * shifted, axis=-1, keepdims=True))
    return (shifted * lax.rsqrt(variance + EPS_LAYER) * gain_vec + bias_vec).astype(jnp.bfloat16)

def attend_group(queries, keys_all, values_all, query_gain, key_gain, heads_total, groups):
    head_size = query_gain.shape[0]
    per_group = heads_total // groups
    seq_count = TOKENS // SEQ_TOKENS
    block_rows = min(512, SEQ_TOKENS)
    position = jnp.arange(SEQ_TOKENS, dtype=jnp.int32)
    score_scale = head_size ** (-0.5)
    query_seq = queries.reshape(seq_count, SEQ_TOKENS, heads_total, head_size)
    key_seq = keys_all.reshape(seq_count, SEQ_TOKENS, groups, head_size)
    value_seq = values_all.reshape(seq_count, SEQ_TOKENS, groups, head_size)

    def one_sequence(operands):
        query_rows, key_rows, value_rows = operands
        rotated_queries = grid_rotate(head_norm(query_rows.astype(jnp.float32), query_gain), position).astype(jnp.bfloat16)
        rotated_keys = grid_rotate(head_norm(key_rows.astype(jnp.float32), key_gain), position).astype(jnp.bfloat16)
        key_float = rotated_keys.astype(jnp.float32)
        value_float = value_rows.astype(jnp.float32)
        blocks = rotated_queries.reshape(SEQ_TOKENS // block_rows, block_rows, groups, per_group, head_size)

        def one_block(query_block):
            scores = jnp.einsum('qgpd,kgd->gpqk', query_block.astype(jnp.float32), key_float) * score_scale
            largest = lax.optimization_barrier(jnp.max(scores, axis=-1, keepdims=True))
            weights = jnp.exp(scores - largest)
            weights = (weights / lax.optimization_barrier(jnp.sum(weights, axis=-1, keepdims=True))).astype(jnp.bfloat16)
            mixed_rows = jnp.einsum('gpqk,kgd->qgpd', weights.astype(jnp.float32), value_float)
            return mixed_rows.astype(jnp.bfloat16)
        mixed_all = lax.map(one_block, blocks)
        return mixed_all.reshape(SEQ_TOKENS, heads_total * head_size)
    result = lax.map(one_sequence, (query_seq, key_seq, value_seq))
    return result.reshape(TOKENS, heads_total * head_size)

def routed_sum(hidden, route_ids, route_weights, expert_gate, expert_up, expert_down):
    assignments = TOKENS * ROUTE_TOP
    most = N_SP * N_TP * CAPACITY
    flat_ids = route_ids.reshape(-1).astype(jnp.int32)
    order = jnp.argsort(flat_ids, stable=True).astype(jnp.int32)
    counts = lax.optimization_barrier(jnp.sum((flat_ids[:, None] == jnp.arange(EXPERTS, dtype=jnp.int32)[None, :]).astype(jnp.int32), axis=0))
    starts = jnp.cumsum(counts) - counts
    slot_rank = jnp.arange(most, dtype=jnp.int32)
    position_in = (starts[:, None] + slot_rank[None, :]).astype(jnp.int32)
    valid = slot_rank[None, :] < counts[:, None]
    picked = jnp.where(valid, order[jnp.minimum(position_in, assignments - 1)], assignments).astype(jnp.int32)
    token_rows = (picked // ROUTE_TOP).astype(jnp.int32)
    padded_hidden = jnp.concatenate([hidden, jnp.zeros((1, MODEL_WIDTH), jnp.bfloat16)], axis=0)
    block_width = EXPERT_WIDTH // N_TP

    def one_expert(operands):
        rows_index, gate_weight, up_weight, down_weight = operands
        rows_in = padded_hidden[rows_index]
        gate_values = jnp.dot(rows_in, gate_weight, preferred_element_type=jnp.float32)
        up_values = jnp.dot(rows_in, up_weight, preferred_element_type=jnp.float32)
        active = (jax.nn.silu(gate_values) * up_values).astype(jnp.bfloat16)
        blocks_in = active.reshape(most, N_TP, block_width).astype(jnp.float32)
        down_blocks = down_weight.reshape(N_TP, block_width, MODEL_WIDTH).astype(jnp.float32)
        partial_value = lax.optimization_barrier(jnp.einsum('mtf,tfd->tmd', blocks_in, down_blocks).astype(jnp.bfloat16))
        return lax.optimization_barrier(jnp.sum(partial_value.astype(jnp.float32), axis=0)).astype(jnp.bfloat16)
    outputs = lax.map(one_expert, (token_rows, expert_gate, expert_up, expert_down))
    padded_weights = jnp.concatenate([route_weights.reshape(-1), jnp.zeros((1,), jnp.float32)], axis=0)
    slot_weight = padded_weights[picked]
    contribution = slot_weight[:, :, None] * outputs.astype(jnp.float32)
    total = jnp.zeros((TOKENS + 1, MODEL_WIDTH), jnp.float32).at[token_rows.reshape(-1)].add(contribution.reshape(-1, MODEL_WIDTH))
    return total[:TOKENS]

def reference(residual, wide_query, narrow_query, wide_keys, narrow_keys, wide_values, narrow_values, wide_query_gain, wide_key_gain, narrow_query_gain, narrow_key_gain, wide_out, narrow_out, first_gain, first_bias, route_ids, route_weights, expert_gate, expert_up, expert_down, shared_gate, shared_up, shared_down, second_gain, second_bias):
    wide_mixed = attend_group(wide_query, wide_keys, wide_values, wide_query_gain, wide_key_gain, WIDE_HEADS, WIDE_GROUPS)
    narrow_mixed = attend_group(narrow_query, narrow_keys, narrow_values, narrow_query_gain, narrow_key_gain, NARROW_HEADS, NARROW_GROUPS)
    projected = jnp.dot(wide_mixed, wide_out, preferred_element_type=jnp.float32) + jnp.dot(narrow_mixed, narrow_out, preferred_element_type=jnp.float32)
    hidden = layer_norm(ALPHA * residual.astype(jnp.float32) + projected, first_gain, first_bias)
    routed = routed_sum(hidden, route_ids, route_weights, expert_gate, expert_up, expert_down)
    shared_gate_values = jnp.dot(hidden, shared_gate, preferred_element_type=jnp.float32)
    shared_up_values = jnp.dot(hidden, shared_up, preferred_element_type=jnp.float32)
    shared_active = (jax.nn.silu(shared_gate_values) * shared_up_values).astype(jnp.bfloat16)
    shared_output = jnp.dot(shared_active, shared_down, preferred_element_type=jnp.float32)
    return layer_norm(ALPHA * hidden.astype(jnp.float32) + routed + shared_output, second_gain, second_bias)
```

```python
import functools
import math

import jax
import jax.numpy as jnp
from jax import lax
from jax.experimental import pallas as pl
from jax.experimental.pallas import tpu as pltpu
from jax.sharding import PartitionSpec as P

WIDE_HEADS = 16
WIDE_GROUPS = 4
NARROW_HEADS = 32
NARROW_GROUPS = 8
GRID_WIDTH = 64
SEQ_SHARDS = 4
LOCAL_EXPERTS = 2


EPS_HEAD = 1e-06
EPS_LAYER = 1e-05
ALPHA = 2.0**0.25
THETA = 10000.0


def swapped(x, axis, apart):
    return lax.ppermute(x, axis, [(i, i ^ 1 << apart) for i in range(lax.axis_size(axis))])


def head_norm(values, gain_vec):
    mean_square = jnp.mean(values * values, axis=-1, keepdims=True)
    return values * lax.rsqrt(mean_square + EPS_HEAD) * gain_vec


def rotate(values, position):
    half_size = values.shape[-1] // 2
    frequency = THETA ** (-jnp.arange(half_size, dtype=jnp.float32) / half_size)
    angles = position.astype(jnp.float32)[:, None] * frequency
    cosine = jnp.cos(angles)[:, None, :]
    sine_part = jnp.sin(angles)[:, None, :]
    leading = values[..., :half_size]
    trailing = values[..., half_size:]
    return jnp.concatenate(
        [leading * cosine - trailing * sine_part, trailing * cosine + leading * sine_part], axis=-1
    )


def grid_rotate(values, position):
    half_size = values.shape[-1] // 2
    grid_row = position // GRID_WIDTH
    grid_col = position % GRID_WIDTH
    return jnp.concatenate(
        [rotate(values[..., :half_size], grid_row), rotate(values[..., half_size:], grid_col)],
        axis=-1,
    )


def layer_norm(values, gain_vec, bias_vec):
    center = jnp.mean(values, axis=-1, keepdims=True)
    shifted = values - center
    variance = jnp.mean(shifted * shifted, axis=-1, keepdims=True)
    return (shifted * lax.rsqrt(variance + EPS_LAYER) * gain_vec + bias_vec).astype(jnp.bfloat16)


def prepare(queries, key_block, value_block, query_gain, key_gain, heads_total, groups, position):
    head_size = query_gain.shape[0]
    local_heads = queries.shape[1] // head_size
    group_index = lax.axis_index("tp") * local_heads // (heads_total // groups)
    query_rows = queries.reshape(queries.shape[0], local_heads, head_size).astype(jnp.float32)
    rotated_queries = grid_rotate(head_norm(query_rows, query_gain), position).astype(jnp.bfloat16)
    column_start = group_index * head_size
    key_rows = lax.dynamic_slice_in_dim(key_block, column_start, head_size, 1).astype(jnp.float32)[
        :, None, :
    ]
    rotated_keys = grid_rotate(head_norm(key_rows, key_gain), position)[:, 0, :].astype(
        jnp.bfloat16
    )
    value_rows = lax.dynamic_slice_in_dim(value_block, column_start, head_size, 1)
    return (rotated_queries, jnp.concatenate([rotated_keys, value_rows], axis=1))


def attend_kernel(query_ref, key_ref, value_ref, mixed_ref, *, factor):
    head_size = query_ref.shape[1]
    scores = lax.dot_general(
        query_ref[...], key_ref[...], (((1,), (1,)), ((), ())), preferred_element_type=jnp.float32
    )
    largest = jnp.max(scores, axis=-1, keepdims=True)
    weights = jnp.exp2((scores - largest) * factor).astype(jnp.bfloat16)
    sums = jnp.dot(weights, value_ref[...], preferred_element_type=jnp.float32)
    mixed_ref[...] = (sums[:, :head_size] / sums[:, head_size : head_size + 1]).astype(jnp.bfloat16)


def attend_local(rotated_queries, key_block, value_block, block_rows=256):
    seg_rows, local_heads, head_size = rotated_queries.shape
    keys = key_block.shape[0]
    rows = seg_rows * local_heads
    block_rows = min(block_rows, rows)
    value_ones = jnp.concatenate(
        [value_block, jnp.ones((keys, 128 - head_size), value_block.dtype)], axis=1
    )
    mixed_rows = pl.pallas_call(
        functools.partial(attend_kernel, factor=math.log2(math.e) * head_size ** (-0.5)),
        out_shape=jax.ShapeDtypeStruct((rows, head_size), jnp.bfloat16),
        grid=(rows // block_rows,),
        in_specs=[
            pl.BlockSpec((block_rows, head_size), lambda i: (i, 0)),
            pl.BlockSpec((keys, head_size), lambda i: (0, 0)),
            pl.BlockSpec((keys, 128), lambda i: (0, 0)),
        ],
        out_specs=pl.BlockSpec((block_rows, head_size), lambda i: (i, 0)),
        cost_estimate=pl.CostEstimate(
            flops=1024 * rows * keys, bytes_accessed=4 * rows * head_size, transcendentals=rows * keys
        ),
        compiler_params=pltpu.CompilerParams(vmem_limit_bytes=60 * 1024 * 1024),
    )(rotated_queries.reshape(rows, head_size), key_block, value_ones)
    return mixed_rows.reshape(seg_rows, local_heads * head_size)


def line_order(place, count, step):
    mirrored = place >= (count + 1) // 2
    near = jnp.where(mirrored, count - 1 - place, place)
    swing = jnp.where(step % 2 == 1, near + (step + 1) // 2, near - step // 2)
    spot = jnp.where(step <= 2 * near, swing, step)
    return jnp.where(mirrored, count - 1 - spot, spot)


def moe_kernel(
    hidden_ref,
    meta_ref,
    gate_hbm,
    up_hbm,
    down_hbm,
    out_ref,
    gate_ref,
    up_ref,
    down_ref,
    hid,
    meta_all,
    rows,
    stage,
    act,
    peer_part,
    ret,
    own_half,
    cross_send,
    cross,
    line_in,
    weight_sem,
    z_send,
    z_recv,
    pair_send,
    pair_recv,
    meta_send,
    meta_recv,
    x_send,
    x_recv,
    rows_send,
    rows_recv,
    part_send,
    part_recv,
    ret_send,
    ret_recv,
    cross_send_sem,
    cross_recv,
    line_send,
    line_recv,
    *,
    n_sp,
    tp_size,
    cap,
    slots,
):
    n_z = tp_size // 2
    tokens, width = hidden_ref.shape
    all_slots = n_sp * slots
    chunk = 512
    me_sp = lax.axis_index("sp")
    me_tp = lax.axis_index("tp")
    z = me_tp // 2
    core = me_tp % 2
    peer = me_tp + 1 - 2 * core

    def remote(src, dst, send_sem, recv_sem, sp, tp):
        return pltpu.make_async_remote_copy(
            src_ref=src,
            dst_ref=dst,
            send_sem=send_sem,
            recv_sem=recv_sem,
            device_id=(sp, tp),
            device_id_type=pl.DeviceIdType.MESH,
        )

    weight_copies = [
        pltpu.make_async_copy(src, dst, weight_sem.at[i])
        for i, (src, dst) in enumerate(
            ((gate_hbm, gate_ref), (up_hbm, up_ref), (down_hbm, down_ref))
        )
    ]

    def up_copy(src, place):
        return remote(src, hid.at[place, core], z_send.at[0, place], z_recv.at[place], me_sp, me_tp + 2)

    def dn_copy(src, place):
        return remote(src, hid.at[place, core], z_send.at[1, place], z_recv.at[place], me_sp, me_tp - 2)

    def pair_copy(src, place):
        return remote(
            src, hid.at[place, core], pair_send.at[place], pair_recv.at[place], me_sp, peer
        )

    def meta_copy(j):
        return remote(
            meta_ref,
            meta_all.at[me_tp],
            meta_send.at[j],
            meta_recv.at[j],
            me_sp,
            (me_tp + j) % tp_size,
        )

    def slot_rows(sp):
        return pl.ds(pl.multiple_of(sp * slots, slots), slots)

    def x_copy(place, j):
        sp = (me_sp + j) % n_sp
        return remote(
            stage.at[place, slot_rows(sp)],
            rows.at[place, core, slot_rows(me_sp)],
            x_send.at[place, j],
            x_recv.at[place, j],
            sp,
            me_tp,
        )

    def rows_copy(place):
        return remote(
            rows.at[place, core],
            rows.at[place, core],
            rows_send.at[place],
            rows_recv.at[place],
            me_sp,
            peer,
        )

    def part_copy(place):
        return remote(
            rows.at[place, 1 - core],
            peer_part.at[place],
            part_send.at[place],
            part_recv.at[place],
            me_sp,
            peer,
        )

    def ret_copy(place, j):
        sp = (me_sp + j) % n_sp
        return remote(
            rows.at[place, core, slot_rows(sp)],
            ret.at[place, slot_rows(me_sp)],
            ret_send.at[place, j],
            ret_recv.at[place, j],
            sp,
            me_tp,
        )

    def cross_copy(place):
        return remote(
            cross_send.at[place],
            cross.at[place],
            cross_send_sem.at[place],
            cross_recv.at[place],
            me_sp,
            peer,
        )

    def line_up(place):
        return remote(
            cross.at[place], line_in.at[place], line_send.at[place], line_recv.at[place], me_sp, me_tp + 2
        )

    def line_dn(place):
        spot = jnp.where(place == z - 1, n_z, place)
        return remote(
            cross.at[place], line_in.at[spot], line_send.at[place], line_recv.at[spot], me_sp, me_tp - 2
        )

    pair_copy(hidden_ref, z).start()

    @pl.when(z < n_z - 1)
    def _():
        up_copy(hidden_ref, z).start()

    @pl.when(z > 0)
    def _():
        dn_copy(hidden_ref, z).start()

    @pl.loop(1, tp_size)
    def _(j):
        meta_copy(j).start()

    for copy in weight_copies:
        copy.start()
    hid[z, core] = hidden_ref[...]
    meta_all[me_tp] = meta_ref[...]

    def selection(place, sp, weighted):
        expert = (LOCAL_EXPERTS * sp + core).astype(jnp.float32)
        parts = []
        for lane in range(2):
            info = meta_all[2 * place + lane]
            line = lax.broadcasted_iota(jnp.int32, (slots, tokens), 0).astype(jnp.float32)
            part = jnp.zeros((slots, tokens), jnp.float32)
            for choice in range(2):
                ids = info[choice : choice + 1, :tokens]
                spots = info[2 + choice : 3 + choice, :tokens] + lane * cap
                target = jnp.where(ids == expert, spots, -1.0)
                value = info[4 + choice : 5 + choice, :tokens] if weighted else 1.0
                part = part + jnp.where(line == target, value, 0.0)
            parts.append(part)
        return jnp.concatenate(parts, axis=1)

    def send_step(step):
        place = line_order(z, n_z, step)

        @pl.when(step > 0)
        def _():
            pltpu.make_async_copy(hidden_ref, hid.at[place, core], z_recv.at[place]).wait()

            @pl.when(jnp.logical_and(place < z, z < n_z - 1))
            def _():
                up_copy(hid.at[place, core], place).start()

            @pl.when(jnp.logical_and(place > z, z > 0))
            def _():
                dn_copy(hid.at[place, core], place).start()

            pair_copy(hid.at[place, core], place).start()

        pltpu.make_async_copy(hidden_ref, hid.at[place, 1 - core], pair_recv.at[place]).wait()
        for lane in range(2):
            j = (me_tp - 2 * place - lane + tp_size) % tp_size

            @pl.when(j > 0)
            def _():
                pltpu.make_async_copy(meta_ref, meta_all.at[2 * place + lane], meta_recv.at[j]).wait()

        @pl.loop(0, n_sp)
        def _(i):
            j = (i + 1) % n_sp
            sp = (me_sp + j) % n_sp
            picks = selection(place, sp, False).astype(jnp.bfloat16)
            for start in range(0, width, chunk):
                piece = (
                    jnp.dot(
                        picks[:, :tokens],
                        hid[place, 0, :, start : start + chunk],
                        preferred_element_type=jnp.float32,
                    )
                    + jnp.dot(
                        picks[:, tokens:],
                        hid[place, 1, :, start : start + chunk],
                        preferred_element_type=jnp.float32,
                    )
                ).astype(jnp.bfloat16)
                stage[place, slot_rows(sp), start : start + chunk] = piece

            @pl.when(j > 0)
            def _():
                x_copy(place, j).start()

            @pl.when(j == 0)
            def _():
                rows[place, core, slot_rows(me_sp)] = stage[place, slot_rows(me_sp)]

    def compute_step(step):
        place = line_order(z, n_z, step)

        @pl.loop(1, n_sp)
        def _(j):
            x_copy(place, j).wait_recv()

        rows_copy(place).start()

        def expert(e):
            block = rows[place, e]
            gate_values = jnp.dot(block, gate_ref[e], preferred_element_type=jnp.float32)
            up_values = jnp.dot(block, up_ref[e], preferred_element_type=jnp.float32)
            act[...] = (jax.nn.silu(gate_values) * up_values).astype(jnp.bfloat16)

        def finish(e):
            for start in range(0, width, chunk):
                rows[place, e, :, start : start + chunk] = jnp.dot(
                    act[...], down_ref[e, :, start : start + chunk], preferred_element_type=jnp.float32
                ).astype(jnp.bfloat16)

        expert(core)
        rows_copy(place).wait()
        finish(core)
        expert(1 - core)
        finish(1 - core)
        part_copy(place).start()

    @pl.loop(0, n_z + 1)
    def _(step):
        @pl.when(step < n_z)
        def _():
            send_step(step)

        @pl.when(step == 1)
        def _():
            for copy in weight_copies:
                copy.wait()

        @pl.when(step > 0)
        def _():
            compute_step(step - 1)

    def return_step(step):
        place = line_order(z, n_z, n_z - 1 - step)
        part_copy(place).wait_recv()

        @pl.loop(0, n_sp)
        def _(i):
            j = (i + 1) % n_sp
            sp = (me_sp + j) % n_sp
            total = (
                rows[place, core, slot_rows(sp)].astype(jnp.float32)
                + peer_part[place, slot_rows(sp)].astype(jnp.float32)
            ).astype(jnp.bfloat16)

            @pl.when(j > 0)
            def _():
                rows[place, core, slot_rows(sp)] = total
                ret_copy(place, j).start()

            @pl.when(j == 0)
            def _():
                ret[place, slot_rows(me_sp)] = total

    def combine_step(step):
        place = line_order(z, n_z, n_z - 1 - step)

        @pl.loop(1, n_sp)
        def _(j):
            ret_copy(place, j).wait_recv()

        for lane in range(2):
            info = meta_all[2 * place + lane]
            lines = lax.broadcasted_iota(jnp.int32, (all_slots, tokens), 0).astype(jnp.float32)
            picks = jnp.zeros((all_slots, tokens), jnp.float32)
            for choice in range(2):
                ids = info[choice : choice + 1, :tokens]
                spots = info[2 + choice : 3 + choice, :tokens] + lane * cap
                shard = jnp.floor(ids * 0.5)
                target = jnp.where(
                    ids - 2.0 * shard == core.astype(jnp.float32), shard * slots + spots, -1.0
                )
                picks = picks + jnp.where(
                    lines == target, info[4 + choice : 5 + choice, :tokens], 0.0
                )
            high = picks.astype(jnp.bfloat16)
            low = (picks - high.astype(jnp.float32)).astype(jnp.bfloat16)

            for start in range(0, width, chunk):
                piece = sum(
                    lax.dot_general(
                        part,
                        ret[place, :, start : start + chunk],
                        (((0,), (0,)), ((), ())),
                        preferred_element_type=jnp.float32,
                    )
                    for part in (high, low)
                )

                @pl.when(core == lane)
                def _():
                    own_half[:, start : start + chunk] = piece

                @pl.when(core != lane)
                def _():
                    cross_send[place, :, start : start + chunk] = piece.astype(jnp.bfloat16)

        cross_copy(place).start()
        cross_copy(place).wait_recv()
        own_half[...] = own_half[...] + cross[place].astype(jnp.float32)

        @pl.when(jnp.logical_and(z > 0, place >= z))
        def _():
            pltpu.make_async_copy(hidden_ref, line_in.at[place], line_recv.at[place]).wait()
            own_half[...] = own_half[...] + line_in[place].astype(jnp.float32)

        @pl.when(jnp.logical_and(z < n_z - 1, place <= z))
        def _():
            spot = jnp.where(place == z, n_z, place)
            pltpu.make_async_copy(hidden_ref, line_in.at[spot], line_recv.at[spot]).wait()
            own_half[...] = own_half[...] + line_in[spot].astype(jnp.float32)

        @pl.when(place == z)
        def _():
            out_ref[...] = own_half[...]

        @pl.when(place > z)
        def _():
            cross[place] = own_half[...].astype(jnp.bfloat16)
            line_up(place).start()

        @pl.when(place < z)
        def _():
            cross[place] = own_half[...].astype(jnp.bfloat16)
            line_dn(place).start()

    @pl.loop(0, n_z + 1)
    def _(step):
        @pl.when(step < n_z)
        def _():
            return_step(step)

        @pl.when(step > 0)
        def _():
            combine_step(step - 1)

    @pl.loop(0, n_z)
    def _(place):
        pair_copy(hidden_ref, place).wait_send()

        @pl.when(jnp.logical_and(place <= z, z < n_z - 1))
        def _():
            up_copy(hidden_ref, place).wait_send()

        @pl.when(jnp.logical_and(place >= z, z > 0))
        def _():
            dn_copy(hidden_ref, place).wait_send()

        part_copy(place).wait_send()
        cross_copy(place).wait_send()

        @pl.when(place != z)
        def _():
            line_up(place).wait_send()

        @pl.loop(1, n_sp)
        def _(j):
            x_copy(place, j).wait_send()
            ret_copy(place, j).wait_send()

    @pl.loop(1, tp_size)
    def _(j):
        meta_copy(j).wait_send()


def moe(hidden, meta, expert_gate, expert_up, expert_down, cap):
    n_sp = lax.axis_size("sp")
    tp_size = lax.axis_size("tp")
    n_z = tp_size // 2
    tokens, width = hidden.shape
    units = expert_gate.shape[2]
    slots = (2 * cap + 15) // 16 * 16
    all_slots = n_sp * slots
    dma = pltpu.SemaphoreType.DMA
    bf16 = jnp.bfloat16
    return pl.pallas_call(
        functools.partial(moe_kernel, n_sp=n_sp, tp_size=tp_size, cap=cap, slots=slots),
        out_shape=jax.ShapeDtypeStruct((tokens, width), jnp.float32),
        in_specs=[pl.BlockSpec(memory_space=pltpu.VMEM)] * 2
        + [pl.BlockSpec(memory_space=pl.ANY)] * 3,
        out_specs=pl.BlockSpec(memory_space=pltpu.VMEM),
        scratch_shapes=[
            pltpu.VMEM((LOCAL_EXPERTS, width, units), bf16),
            pltpu.VMEM((LOCAL_EXPERTS, width, units), bf16),
            pltpu.VMEM((LOCAL_EXPERTS, units, width), bf16),
            pltpu.VMEM((n_z, 2, tokens, width), bf16),
            pltpu.VMEM((tp_size, 8, 128), jnp.float32),
            pltpu.VMEM((n_z, LOCAL_EXPERTS, all_slots, width), bf16),
            pltpu.VMEM((n_z, all_slots, width), bf16),
            pltpu.VMEM((all_slots, units), bf16),
            pltpu.VMEM((n_z, all_slots, width), bf16),
            pltpu.VMEM((n_z, all_slots, width), bf16),
            pltpu.VMEM((tokens, width), jnp.float32),
            pltpu.VMEM((n_z, tokens, width), bf16),
            pltpu.VMEM((n_z, tokens, width), bf16),
            pltpu.VMEM((n_z + 1, tokens, width), bf16),
            dma((3,)),
            dma((2, n_z)),
            dma((n_z,)),
            dma((n_z,)),
            dma((n_z,)),
            dma((tp_size,)),
            dma((tp_size,)),
            dma((n_z, n_sp)),
            dma((n_z, n_sp)),
            dma((n_z,)),
            dma((n_z,)),
            dma((n_z,)),
            dma((n_z,)),
            dma((n_z, n_sp)),
            dma((n_z, n_sp)),
            dma((n_z,)),
            dma((n_z,)),
            dma((n_z,)),
            dma((n_z + 1,)),
        ],
        compiler_params=pltpu.CompilerParams(
            has_side_effects=True, vmem_limit_bytes=67_000_000
        ),
    )(hidden, meta, expert_gate, expert_up, expert_down)


def local(
    residual,
    wide_query,
    narrow_query,
    wide_keys,
    narrow_keys,
    wide_values,
    narrow_values,
    wide_query_gain,
    wide_key_gain,
    narrow_query_gain,
    narrow_key_gain,
    wide_out,
    narrow_out,
    first_gain,
    first_bias,
    route_ids,
    route_weights,
    expert_gate,
    expert_up,
    expert_down,
    shared_gate,
    shared_up,
    shared_down,
    second_gain,
    second_bias,
):
    seg_rows = wide_query.shape[0]
    position = lax.axis_index("sp") % SEQ_SHARDS * seg_rows + jnp.arange(seg_rows, dtype=jnp.int32)
    wide_rotated, wide_pack = prepare(
        wide_query,
        wide_keys,
        wide_values,
        wide_query_gain,
        wide_key_gain,
        WIDE_HEADS,
        WIDE_GROUPS,
        position,
    )
    narrow_rotated, narrow_pack = prepare(
        narrow_query,
        narrow_keys,
        narrow_values,
        narrow_query_gain,
        narrow_key_gain,
        NARROW_HEADS,
        NARROW_GROUPS,
        position,
    )
    gathered = jnp.concatenate([wide_pack, narrow_pack], axis=1)
    for level in range(SEQ_SHARDS.bit_length() - 1):
        partner = swapped(gathered, "sp", level)
        is_upper = lax.axis_index("sp") // 2**level % 2 == 1
        gathered = jnp.where(
            is_upper,
            jnp.concatenate([partner, gathered], axis=0),
            jnp.concatenate([gathered, partner], axis=0),
        )
    wide_size = wide_query_gain.shape[0]
    narrow_size = narrow_query_gain.shape[0]
    narrow_start = 2 * wide_size
    wide_mixed = attend_local(
        wide_rotated, gathered[:, :wide_size], gathered[:, wide_size:narrow_start]
    )
    narrow_mixed = attend_local(
        narrow_rotated,
        gathered[:, narrow_start : narrow_start + narrow_size],
        gathered[:, narrow_start + narrow_size :],
    )
    wide_tokens, narrow_tokens = (
        lax.all_to_all(wide_mixed, "tp", split_axis=0, concat_axis=1, tiled=True),
        lax.all_to_all(narrow_mixed, "tp", split_axis=0, concat_axis=1, tiled=True),
    )
    running = jnp.dot(
        wide_tokens,
        lax.all_gather(wide_out, "tp", axis=0, tiled=True),
        preferred_element_type=jnp.float32,
    )
    projected = running + jnp.dot(
        narrow_tokens,
        lax.all_gather(narrow_out, "tp", axis=0, tiled=True),
        preferred_element_type=jnp.float32,
    )
    hidden = layer_norm(ALPHA * residual.astype(jnp.float32) + projected, first_gain, first_bias)
    device_rows = hidden.shape[0]
    sp_size = lax.axis_size("sp")
    top_count = route_ids.shape[1]
    experts = LOCAL_EXPERTS * sp_size
    capacity = max(2, (5 * device_rows * top_count + 4 * experts - 1) // (4 * experts))
    flat_ids = route_ids.reshape(-1)
    expert_hits = (flat_ids[:, None] == jnp.arange(experts, dtype=jnp.int32)[None, :]).astype(
        jnp.int32
    )
    earlier = jnp.sum((jnp.cumsum(expert_hits, axis=0) - expert_hits) * expert_hits, axis=1)
    meta = jnp.concatenate(
        [
            route_ids.T.astype(jnp.float32),
            earlier.reshape(device_rows, top_count).T.astype(jnp.float32),
            route_weights.T,
            jnp.zeros((8 - 3 * top_count, device_rows), jnp.float32),
        ],
        axis=0,
    )
    meta = jnp.pad(meta, ((0, 0), (0, max(0, 128 - device_rows))))
    routed = moe(hidden, meta, expert_gate, expert_up, expert_down, capacity)
    shared_gate_values = jnp.dot(hidden, shared_gate, preferred_element_type=jnp.float32)
    shared_up_values = jnp.dot(hidden, shared_up, preferred_element_type=jnp.float32)
    shared_active = (jax.nn.silu(shared_gate_values) * shared_up_values).astype(jnp.bfloat16)
    shared_output = jnp.dot(shared_active, shared_down, preferred_element_type=jnp.float32)
    return layer_norm(
        ALPHA * hidden.astype(jnp.float32) + routed + shared_output, second_gain, second_bias
    )


def solution(mesh):
    in_specs = (
        P(("sp", "tp"), None),
        P("sp", "tp"),
        P("sp", "tp"),
        P("sp", None),
        P("sp", None),
        P("sp", None),
        P("sp", None),
        P(),
        P(),
        P(),
        P(),
        P("tp", None),
        P("tp", None),
        P(),
        P(),
        P(("sp", "tp"), None),
        P(("sp", "tp"), None),
        P("sp", None, "tp"),
        P("sp", None, "tp"),
        P("sp", "tp", None),
        P(),
        P(),
        P(),
        P(),
        P(),
    )
    out_specs = P(("sp", "tp"), None)
    return jax.shard_map(local, mesh=mesh, in_specs=in_specs, out_specs=out_specs, check_vma=False)
```

```python
import functools
import math

import jax
import jax.numpy as jnp
import numpy as np
from jax import lax
from jax.experimental import pallas as pl
from jax.experimental.pallas import tpu as pltpu
from jax.sharding import PartitionSpec as P

WIDE_HEADS = 16
WIDE_GROUPS = 4
NARROW_HEADS = 32
NARROW_GROUPS = 8
GRID_WIDTH = 64
SEQ_SHARDS = 4
LOCAL_EXPERTS = 2


EPS_HEAD = 1e-06
EPS_LAYER = 1e-05
ALPHA = 2.0**0.25
THETA = 10000.0


def line_order(place, count, step):
    mirrored = place >= (count + 1) // 2
    near = jnp.where(mirrored, count - 1 - place, place)
    swing = jnp.where(step % 2 == 1, near + (step + 1) // 2, near - step // 2)
    spot = jnp.where(step <= 2 * near, swing, step)
    return jnp.where(mirrored, count - 1 - spot, spot)


def angle_tables(head_size, lanes, grid_rows):
    half, quarter = head_size // 2, head_size // 4
    lane = np.arange(lanes)
    spot = lane % half
    frequency = THETA ** (-(spot % quarter) / quarter)
    by_row = lane % head_size < half
    sign = np.where(spot < quarter, -1.0, 1.0)
    angles = np.arange(max(grid_rows, GRID_WIDTH))[:, None] * frequency[None, :]
    tables = []
    for keep, count in ((by_row, grid_rows), (~by_row, GRID_WIDTH)):
        tables.append(np.where(keep, np.cos(angles[:count]), 0.0))
        tables.append(np.where(keep, sign * np.sin(angles[:count]), 0.0))
    return [table.astype(np.float32) for table in tables]


def attention_kernel(
    wide_query,
    narrow_query,
    wide_keys,
    narrow_keys,
    wide_values,
    narrow_values,
    gains,
    wide_row_cos,
    wide_row_sin,
    wide_col_cos,
    wide_col_sin,
    narrow_row_cos,
    narrow_row_sin,
    narrow_col_cos,
    narrow_col_sin,
    residual,
    wide_out,
    narrow_out,
    norm_gain,
    norm_bias,
    hidden_ref,
    wide_kv,
    narrow_kv,
    values_ones,
    wide_heads,
    narrow_heads,
    out_all,
    mixed,
    gathered,
    projected,
    load_sem,
    kv_send,
    kv_recv,
    kv_pair_send,
    kv_pair_recv,
    line_send,
    line_recv,
    out_pair_send,
    out_pair_recv,
    share_send,
    share_recv,
    mixed_send,
    mixed_recv,
    *,
    tp_size,
    shards,
    wide_size,
    narrow_size,
    local_wide,
    local_narrow,
):
    n_z = tp_size // 2
    lanes = 128
    tokens, width = residual.shape
    seg_rows = wide_query.shape[0]
    half_rows = seg_rows // 2
    prep_rows = 256
    prep_grid = prep_rows // GRID_WIDTH
    out_rows = wide_out.shape[0]
    piece = 2 * out_rows // shards
    me_sp = lax.axis_index("sp")
    me_tp = lax.axis_index("tp")
    z = me_tp // 2
    core = me_tp % 2
    peer = me_tp + 1 - 2 * core
    shard = me_sp % shards
    first_sp = me_sp - shard
    kinds = (wide_kv, narrow_kv)

    def remote(src, dst, send_sem, recv_sem, sp, tp):
        return pltpu.make_async_remote_copy(
            src_ref=src,
            dst_ref=dst,
            send_sem=send_sem,
            recv_sem=recv_sem,
            device_id=(sp, tp),
            device_id_type=pl.DeviceIdType.MESH,
        )

    def kv_part(kind, owner, side):
        start = pl.multiple_of(owner * seg_rows + side * half_rows, half_rows)
        return kinds[kind].at[pl.ds(start, half_rows)]

    def kv_copy(kind, j):
        part = kv_part(kind, shard, core)
        return remote(
            part, part, kv_send.at[kind, j], kv_recv.at[kind, j], first_sp + (shard + j) % shards, me_tp
        )

    def kv_pair(kind, j):
        part = kv_part(kind, (shard - j + shards) % shards, core)
        return remote(
            part, part, kv_pair_send.at[kind, j], kv_pair_recv.at[kind, j], me_sp, peer
        )

    def out_piece(place, owner):
        return out_all.at[2 * place + core, pl.ds(pl.multiple_of(owner * piece, piece), piece)]

    def line_copy(way, d):
        part = out_piece(z, shard)
        return remote(
            part, part, line_send.at[way, d], line_recv.at[z], me_sp, me_tp + (2 - 4 * way) * d
        )

    def out_pair(place, j):
        part = out_piece(place, (shard - j + shards) % shards)
        return remote(part, part, out_pair_send.at[place, j], out_pair_recv.at[place, j], me_sp, peer)

    def own_pair():
        part = out_all.at[me_tp]
        return remote(part, part, out_pair_send.at[z, 0], out_pair_recv.at[z, 0], me_sp, peer)

    def share_copy(place, j):
        part = out_piece(place, shard)
        return remote(
            part, part, share_send.at[place, j], share_recv.at[place, j],
            first_sp + (shard + j) % shards, me_tp,
        )

    def mixed_copy(kind, b):
        target = (me_tp + 1 + b) % tp_size
        return remote(
            mixed.at[kind, target],
            gathered.at[me_tp, :, pl.ds(kind * lanes, lanes)],
            mixed_send.at[kind, b],
            mixed_recv.at[kind, b],
            me_sp,
            target,
        )

    loads = [
        pltpu.make_async_copy(
            src, out_all.at[me_tp, pl.ds(i * out_rows, out_rows)], load_sem.at[i]
        )
        for i, src in enumerate((wide_out, narrow_out))
    ]
    for copy in loads:
        copy.start()

    lane = lax.broadcasted_iota(jnp.int32, (1, lanes), 1)

    def normalized(values, size, gain_row, row_cos, row_sin, col_cos, col_sin, i):
        squares = values * values
        high = squares.astype(jnp.bfloat16)
        low = (squares - high.astype(jnp.float32)).astype(jnp.bfloat16)
        left = lax.broadcasted_iota(jnp.int32, (lanes, lanes), 0) // size
        right = lax.broadcasted_iota(jnp.int32, (lanes, lanes), 1) // size
        same = jnp.where(left == right, 1.0, 0.0).astype(jnp.bfloat16)
        total = jnp.dot(high, same, preferred_element_type=jnp.float32) + jnp.dot(
            low, same, preferred_element_type=jnp.float32
        )
        scaled = values * lax.rsqrt(total * (1.0 / size) + EPS_HEAD) * gains[gain_row : gain_row + 1, :]
        quarter = size // 4
        partner = jnp.where(
            lane % (size // 2) < quarter,
            pltpu.roll(scaled, lanes - quarter, 1),
            pltpu.roll(scaled, quarter, 1),
        )
        grid_row = (shard * (seg_rows // prep_rows) + i) * prep_grid

        def spread(by_row, by_col):
            lines = by_row[pl.ds(grid_row, prep_grid), :]
            return jnp.concatenate([lines[g : g + 1, :] + by_col[...] for g in range(prep_grid)], axis=0)

        return scaled * spread(row_cos, col_cos) + partner * spread(row_sin, col_sin)

    wide_tables = (wide_row_cos, wide_row_sin, wide_col_cos, wide_col_sin)
    narrow_tables = (narrow_row_cos, narrow_row_sin, narrow_col_cos, narrow_col_sin)

    def column_pick(source, group, size):
        column = lax.broadcasted_iota(jnp.int32, (source.shape[1], lanes), 0)
        return jnp.where(column == group * size + lane % size, 1.0, 0.0).astype(jnp.bfloat16)

    def key_step(kind, i, keys, values, picks, size, gain_row, tables):
        rows = pl.ds(pl.multiple_of(i * prep_rows, prep_rows), prep_rows)
        own_keys = jnp.dot(keys[rows, :], picks, preferred_element_type=jnp.float32)
        own_values = jnp.dot(values[rows, :], picks, preferred_element_type=jnp.float32)
        rotated = normalized(own_keys, size, gain_row, *tables, i)
        packed = jnp.where((lane // size) % 2 == 0, rotated, own_values).astype(jnp.bfloat16)
        start = pl.multiple_of(shard * seg_rows + i * prep_rows, prep_rows)
        kinds[kind][pl.ds(start, prep_rows), :] = packed

    per_wide = WIDE_HEADS // WIDE_GROUPS
    per_narrow = NARROW_HEADS // NARROW_GROUPS
    wide_picks = column_pick(wide_keys, me_tp * local_wide // per_wide, wide_size)
    lower_group = 2 * z * local_narrow // per_narrow
    upper_group = (2 * z + 1) * local_narrow // per_narrow
    narrow_picks = column_pick(
        narrow_keys, jnp.where(lane < lanes // 2, lower_group, upper_group), narrow_size
    )
    blocks = seg_rows // prep_rows

    @pl.loop(0, blocks)
    def _(i):
        key_step(0, i, wide_keys, wide_values, wide_picks, wide_size, 1, wide_tables)

    for j in range(1, shards):
        kv_copy(0, j).start()

    for copy in loads:
        copy.wait()
    own_pair().start()

    for d in range(1, n_z):

        @pl.when(z + d < n_z)
        def _():
            line_copy(0, d).start()

        @pl.when(z - d >= 0)
        def _():
            line_copy(1, d).start()

    @pl.loop(0, blocks)
    def _(i):
        key_step(1, i, narrow_keys, narrow_values, narrow_picks, narrow_size, 3, narrow_tables)

    for j in range(1, shards):
        kv_copy(1, j).start()
    @pl.loop(0, blocks)
    def _(i):
        rows = pl.ds(pl.multiple_of(i * prep_rows, prep_rows), prep_rows)
        rotated = normalized(
            wide_query[rows, :].astype(jnp.float32), wide_size, 0, *wide_tables, i
        )
        for h in range(local_wide):
            moved = rotated if h == 0 else pltpu.roll(rotated, lanes - h * wide_size, 1)
            wide_heads[h, rows] = jnp.where(lane < wide_size, moved, 0.0).astype(jnp.bfloat16)
        rotated = normalized(
            narrow_query[rows, :].astype(jnp.float32), narrow_size, 2, *narrow_tables, i
        )
        for h in range(local_narrow):
            shift = (core * (lanes // 2) + lanes - h * narrow_size) % lanes
            moved = pltpu.roll(rotated, shift, 1)
            kept = lane // narrow_size == 2 * core
            narrow_heads[h, rows] = jnp.where(kept, moved, 0.0).astype(jnp.bfloat16)

    def attend(block, kv, size):
        scores = lax.dot_general(
            block, kv[...], (((1,), (1,)), ((), ())), preferred_element_type=jnp.float32
        )
        largest = jnp.max(scores, axis=-1, keepdims=True)
        factor = math.log2(math.e) * size ** (-0.5)
        weights = jnp.exp2((scores - largest) * factor).astype(jnp.bfloat16)
        sums = jnp.dot(weights, values_ones[...], preferred_element_type=jnp.float32)
        return sums / sums[:, 0:1]

    def relay_kv(kind):
        for j in range(1, shards):
            kv_copy(kind, j).wait_recv()
            kv_pair(kind, j).start()
        for j in range(1, shards):
            kv_pair(kind, j).wait_recv()
        size = (wide_size, narrow_size)[kind]
        keep = jnp.where((lane // size) % 2 == 1, 1.0, 0.0).astype(jnp.bfloat16)
        fill = jnp.where((lane // size) % 2 == 1, 0.0, 1.0).astype(jnp.bfloat16)

        @pl.loop(0, shards * blocks)
        def _(i):
            rows = pl.ds(pl.multiple_of(i * prep_rows, prep_rows), prep_rows)
            values_ones[rows, :] = kinds[kind][rows, :] * keep + fill

    def put_mixed(kind, b, target, value):
        @pl.when(b < tp_size - 1)
        def _():
            mixed[kind, target] = value
            mixed_copy(kind, b).start()

        @pl.when(b == tp_size - 1)
        def _():
            gathered[target, :, kind * lanes : (kind + 1) * lanes] = value

    def share_step(step):
        place = line_order(z, n_z, step)
        part = out_piece(place, shard)
        pltpu.make_async_copy(part, part, line_recv.at[place]).wait()
        for j in range(1, shards):
            share_copy(place, j).start()
        out_pair(place, 0).start()

    early = (tp_size - tp_size // 2 + 2) // 3
    relay_kv(0)

    @pl.loop(0, tp_size)
    def _(b):
        @pl.when(jnp.logical_and(b >= tp_size // 2, (b - tp_size // 2) % 3 == 0))
        def _():
            share_step((b - tp_size // 2) // 3 + 1)

        target = (me_tp + 1 + b) % tp_size
        rows = pl.ds(pl.multiple_of(target * tokens, tokens), tokens)
        block = jnp.concatenate([wide_heads[h, rows] for h in range(local_wide)], axis=0)
        values = attend(block, wide_kv, wide_size)
        total = jnp.zeros((tokens, lanes), jnp.float32)
        for h in range(local_wide):
            part = values[h * tokens : (h + 1) * tokens]
            shift = ((h + 1) * wide_size) % lanes
            moved = part if shift == 0 else pltpu.roll(part, shift, 1)
            total = total + jnp.where(lane // wide_size == h, moved, 0.0)
        put_mixed(0, b, target, total.astype(jnp.bfloat16))

    relay_kv(1)

    @pl.loop(0, tp_size)
    def _(b):
        @pl.when(jnp.logical_and(b > 0, b + early < n_z))
        def _():
            share_step(b + early)

        @pl.when(b > tp_size - n_z)
        def _():
            place = line_order(z, n_z, b - (tp_size - n_z))
            for j in range(1, shards):
                share_copy(place, j).wait_recv()
                out_pair(place, j).start()

        target = (me_tp + 1 + b) % tp_size
        rows = pl.ds(pl.multiple_of(target * tokens, tokens), tokens)
        total = jnp.zeros((tokens, lanes), jnp.float32)
        for first in range(0, local_narrow, 2):
            block = jnp.concatenate([narrow_heads[first + h, rows] for h in range(2)], axis=0)
            values = attend(block, narrow_kv, narrow_size)
            for h in range(2):
                part = values[h * tokens : (h + 1) * tokens]
                shift = (
                    (first + h) * narrow_size + 2 * lanes - core * (lanes // 2) - narrow_size
                ) % lanes
                moved = pltpu.roll(part, shift, 1)
                total = total + jnp.where(lane // narrow_size == first + h, moved, 0.0)
        put_mixed(1, b, target, total.astype(jnp.bfloat16))

    @pl.loop(0, n_z)
    def _(place):
        @pl.when(place == z)
        def _():
            own_pair().wait_recv()

        @pl.when(place != z)
        def _():
            for j in range(shards):
                out_pair(place, j).wait_recv()

    @pl.loop(0, tp_size - 1)
    def _(b):
        mixed_copy(0, b).wait_recv()
        mixed_copy(1, b).wait_recv()

    chunk = 512
    for start in range(0, width, chunk):

        def add(q, total):
            if out_rows == lanes:
                return total + jnp.dot(
                    gathered[q],
                    out_all[q, :, start : start + chunk],
                    preferred_element_type=jnp.float32,
                )
            for kind in range(2):
                total = total + jnp.dot(
                    gathered[q, :, kind * lanes : kind * lanes + out_rows],
                    out_all[q, kind * out_rows : (kind + 1) * out_rows, start : start + chunk],
                    preferred_element_type=jnp.float32,
                )
            return total

        projected[:, start : start + chunk] = lax.fori_loop(
            0, tp_size, add, ALPHA * residual[:, start : start + chunk].astype(jnp.float32)
        )

    values = projected[...]
    center = jnp.mean(values, axis=-1, keepdims=True)
    shifted = values - center
    variance = jnp.mean(shifted * shifted, axis=-1, keepdims=True)
    hidden_ref[...] = (
        shifted * lax.rsqrt(variance + EPS_LAYER) * norm_gain[...] + norm_bias[...]
    ).astype(jnp.bfloat16)

    own_pair().wait_send()
    for j in range(1, shards):
        for kind in range(2):
            kv_copy(kind, j).wait_send()
            kv_pair(kind, j).wait_send()

    @pl.loop(0, n_z)
    def _(place):
        @pl.when(jnp.logical_and(place > 0, z + place < n_z))
        def _():
            line_copy(0, place).wait_send()

        @pl.when(jnp.logical_and(place > 0, z - place >= 0))
        def _():
            line_copy(1, place).wait_send()

        @pl.when(place != z)
        def _():
            for j in range(shards):
                out_pair(place, j).wait_send()
            for j in range(1, shards):
                share_copy(place, j).wait_send()

    @pl.loop(0, tp_size - 1)
    def _(b):
        mixed_copy(0, b).wait_send()
        mixed_copy(1, b).wait_send()


def attention(
    queries, keys_values, gain_vecs, residual, wide_out, narrow_out, first_gain, first_bias
):
    tp_size = lax.axis_size("tp")
    n_z = tp_size // 2
    lanes = 128
    tokens, width = residual.shape
    seg_rows = queries[0].shape[0]
    shards = SEQ_SHARDS
    sizes = gain_vecs[0].shape[0], gain_vecs[2].shape[0]
    local_heads = [q.shape[1] // size for q, size in zip(queries, sizes)]
    queries = [jnp.pad(q, ((0, 0), (0, lanes - q.shape[1]))) for q in queries]
    gains = jnp.concatenate(
        [gain for gain in gain_vecs for _ in range(lanes // gain.shape[0])]
    ).reshape(len(gain_vecs), lanes)
    grid_rows = shards * seg_rows // GRID_WIDTH
    tables = [
        jnp.asarray(table)
        for size in sizes
        for table in angle_tables(size, lanes, grid_rows)
    ]
    bf16 = jnp.bfloat16
    dma = pltpu.SemaphoreType.DMA
    vmem = pl.BlockSpec(memory_space=pltpu.VMEM)
    hbm = pl.BlockSpec(memory_space=pl.ANY)
    return pl.pallas_call(
        functools.partial(
            attention_kernel,
            tp_size=tp_size,
            shards=shards,
            wide_size=sizes[0],
            narrow_size=sizes[1],
            local_wide=local_heads[0],
            local_narrow=local_heads[1],
        ),
        out_shape=jax.ShapeDtypeStruct((tokens, width), bf16),
        in_specs=[vmem] * 16 + [hbm] * 2 + [vmem] * 2,
        out_specs=vmem,
        scratch_shapes=[
            pltpu.VMEM((shards * seg_rows, lanes), bf16),
            pltpu.VMEM((shards * seg_rows, lanes), bf16),
            pltpu.VMEM((shards * seg_rows, lanes), bf16),
            pltpu.VMEM((local_heads[0], seg_rows, lanes), bf16),
            pltpu.VMEM((local_heads[1], seg_rows, lanes), bf16),
            pltpu.VMEM((tp_size, 2 * wide_out.shape[0], width), bf16),
            pltpu.VMEM((2, tp_size, tokens, lanes), bf16),
            pltpu.VMEM((tp_size, tokens, 2 * lanes), bf16),
            pltpu.VMEM((tokens, width), jnp.float32),
            dma((2,)),
            dma((2, shards)),
            dma((2, shards)),
            dma((2, shards)),
            dma((2, shards)),
            dma((2, n_z)),
            dma((n_z,)),
            dma((n_z, shards)),
            dma((n_z, shards)),
            dma((n_z, shards)),
            dma((n_z, shards)),
            dma((2, tp_size)),
            dma((2, tp_size)),
        ],
        compiler_params=pltpu.CompilerParams(
            has_side_effects=True, vmem_limit_bytes=66_000_000
        ),
    )(
        *queries,
        *keys_values,
        gains,
        *tables,
        residual,
        wide_out,
        narrow_out,
        first_gain.reshape(1, width),
        first_bias.reshape(1, width),
    )


def moe_kernel(
    hidden_ref,
    meta_ref,
    shared_gate,
    shared_up,
    shared_down,
    norm_gain,
    norm_bias,
    gate_hbm,
    up_hbm,
    down_hbm,
    out_ref,
    gate_ref,
    up_ref,
    down_ref,
    hid,
    meta_all,
    rows,
    stage,
    act,
    peer_part,
    ret,
    own_half,
    result,
    spots_all,
    cross_send,
    cross,
    line_in,
    weight_sem,
    z_send,
    z_recv,
    pair_send,
    pair_recv,
    meta_send,
    meta_recv,
    x_send,
    x_recv,
    rows_send,
    rows_recv,
    part_send,
    part_recv,
    ret_send,
    ret_recv,
    cross_send_sem,
    cross_recv,
    line_send,
    line_recv,
    *,
    n_sp,
    tp_size,
    cap,
    slots,
):
    n_z = tp_size // 2
    tokens, width = hidden_ref.shape
    all_slots = n_sp * slots
    chunk = 512
    expert_lines = (LOCAL_EXPERTS * n_sp + 15) // 16 * 16
    me_sp = lax.axis_index("sp")
    me_tp = lax.axis_index("tp")
    z = me_tp // 2
    core = me_tp % 2
    peer = me_tp + 1 - 2 * core

    def remote(src, dst, send_sem, recv_sem, sp, tp):
        return pltpu.make_async_remote_copy(
            src_ref=src,
            dst_ref=dst,
            send_sem=send_sem,
            recv_sem=recv_sem,
            device_id=(sp, tp),
            device_id_type=pl.DeviceIdType.MESH,
        )

    weight_copies = [
        pltpu.make_async_copy(src, dst, weight_sem.at[i])
        for i, (src, dst) in enumerate(
            ((gate_hbm, gate_ref), (up_hbm, up_ref), (down_hbm, down_ref))
        )
    ]

    def line_copy(src, way, place):
        return remote(
            src,
            hid.at[place, core],
            z_send.at[way, place],
            z_recv.at[place],
            me_sp,
            me_tp + 2 - 4 * way,
        )

    def pair_copy(src, place):
        return remote(
            src, hid.at[place, core], pair_send.at[place], pair_recv.at[place], me_sp, peer
        )

    def meta_copy(j):
        return remote(
            meta_ref,
            meta_all.at[me_tp],
            meta_send.at[j],
            meta_recv.at[j],
            me_sp,
            (me_tp + j) % tp_size,
        )

    def slot_rows(sp):
        return pl.ds(pl.multiple_of(sp * slots, slots), slots)

    def x_copy(place, j):
        sp = (me_sp + j) % n_sp
        return remote(
            stage.at[place, slot_rows(sp)],
            rows.at[place, core, slot_rows(me_sp)],
            x_send.at[place, j],
            x_recv.at[place, j],
            sp,
            me_tp,
        )

    def rows_copy(place):
        return remote(
            rows.at[place, core],
            rows.at[place, core],
            rows_send.at[place],
            rows_recv.at[place],
            me_sp,
            peer,
        )

    def part_copy(place):
        return remote(
            rows.at[place, 1 - core],
            peer_part.at[place],
            part_send.at[place],
            part_recv.at[place],
            me_sp,
            peer,
        )

    def ret_copy(place, j):
        sp = (me_sp + j) % n_sp
        return remote(
            rows.at[place, core, slot_rows(sp)],
            ret.at[place, slot_rows(me_sp)],
            ret_send.at[place, j],
            ret_recv.at[place, j],
            sp,
            me_tp,
        )

    def cross_copy(place):
        return remote(
            cross_send.at[place],
            cross.at[place],
            cross_send_sem.at[place],
            cross_recv.at[place],
            me_sp,
            peer,
        )

    def line_up(place):
        return remote(
            cross.at[place], line_in.at[place], line_send.at[place], line_recv.at[place], me_sp, me_tp + 2
        )

    def line_dn(place):
        spot = jnp.where(place == z - 1, n_z, place)
        return remote(
            cross.at[place], line_in.at[spot], line_send.at[place], line_recv.at[spot], me_sp, me_tp - 2
        )

    pair_copy(hidden_ref, z).start()

    @pl.when(z < n_z - 1)
    def _():
        line_copy(hidden_ref, 0, z).start()

    @pl.when(z > 0)
    def _():
        line_copy(hidden_ref, 1, z).start()

    @pl.loop(1, tp_size)
    def _(j):
        meta_copy(j).start()

    for copy in weight_copies:
        copy.start()
    hid[z, core] = hidden_ref[...]
    meta_all[me_tp] = meta_ref[...]

    def selection(place, sp, weighted):
        expert = (LOCAL_EXPERTS * sp + core).astype(jnp.float32)
        parts = []
        for lane in range(2):
            info = meta_all[2 * place + lane]
            line = lax.broadcasted_iota(jnp.int32, (slots, tokens), 0).astype(jnp.float32)
            part = jnp.zeros((slots, tokens), jnp.float32)
            for choice in range(2):
                ids = info[choice : choice + 1, :tokens]
                spots = spots_all[2 * place + lane, choice : choice + 1, :tokens] + lane * cap
                target = jnp.where(ids == expert, spots, -1.0)
                value = info[2 + choice : 3 + choice, :tokens] if weighted else 1.0
                part = part + jnp.where(line == target, value, 0.0)
            parts.append(part)
        return jnp.concatenate(parts, axis=1)

    def shared_expert():
        gate_values = jnp.dot(hidden_ref[...], shared_gate[...], preferred_element_type=jnp.float32)
        up_values = jnp.dot(hidden_ref[...], shared_up[...], preferred_element_type=jnp.float32)
        active = (jax.nn.silu(gate_values) * up_values).astype(jnp.bfloat16)
        for start in range(0, width, chunk):
            cols = slice(start, start + chunk)
            result[:, cols] = ALPHA * hidden_ref[:, cols].astype(jnp.float32) + jnp.dot(
                active, shared_down[:, cols], preferred_element_type=jnp.float32
            )

    def send_step(step):
        place = line_order(z, n_z, step)

        @pl.when(step > 0)
        def _():
            pltpu.make_async_copy(hidden_ref, hid.at[place, core], z_recv.at[place]).wait()

            @pl.when(jnp.logical_and(place < z, z < n_z - 1))
            def _():
                line_copy(hid.at[place, core], 0, place).start()

            @pl.when(jnp.logical_and(place > z, z > 0))
            def _():
                line_copy(hid.at[place, core], 1, place).start()

            pair_copy(hid.at[place, core], place).start()

        pltpu.make_async_copy(hidden_ref, hid.at[place, 1 - core], pair_recv.at[place]).wait()
        for lane in range(2):
            j = (me_tp - 2 * place - lane + tp_size) % tp_size

            @pl.when(j > 0)
            def _():
                pltpu.make_async_copy(meta_ref, meta_all.at[2 * place + lane], meta_recv.at[j]).wait()

            info = meta_all[2 * place + lane]
            line = lax.broadcasted_iota(jnp.int32, (expert_lines, 128), 0).astype(jnp.float32)
            first = jnp.where(line == info[0:1, :], 1.0, 0.0)
            second = jnp.where(line == info[1:2, :], 1.0, 0.0)
            before = lax.broadcasted_iota(jnp.int32, (128, 128), 0) < lax.broadcasted_iota(
                jnp.int32, (128, 128), 1
            )
            counts = jnp.dot(
                (first + second).astype(jnp.bfloat16),
                jnp.where(before, 1.0, 0.0).astype(jnp.bfloat16),
                preferred_element_type=jnp.float32,
            )
            spots_all[2 * place + lane, 0:1] = jnp.sum(first * counts, axis=0, keepdims=True)
            spots_all[2 * place + lane, 1:2] = jnp.sum(second * counts, axis=0, keepdims=True)

        @pl.loop(0, n_sp)
        def _(i):
            j = (i + 1) % n_sp
            sp = (me_sp + j) % n_sp
            picks = selection(place, sp, False).astype(jnp.bfloat16)
            for start in range(0, width, chunk):
                piece = (
                    jnp.dot(
                        picks[:, :tokens],
                        hid[place, 0, :, start : start + chunk],
                        preferred_element_type=jnp.float32,
                    )
                    + jnp.dot(
                        picks[:, tokens:],
                        hid[place, 1, :, start : start + chunk],
                        preferred_element_type=jnp.float32,
                    )
                ).astype(jnp.bfloat16)
                stage[place, slot_rows(sp), start : start + chunk] = piece

            @pl.when(j > 0)
            def _():
                x_copy(place, j).start()

            @pl.when(j == 0)
            def _():
                rows[place, core, slot_rows(me_sp)] = stage[place, slot_rows(me_sp)]

    def compute_step(step):
        place = line_order(z, n_z, step)

        @pl.loop(1, n_sp)
        def _(j):
            x_copy(place, j).wait_recv()

        rows_copy(place).start()

        def expert(e):
            block = rows[place, e]
            gate_values = jnp.dot(block, gate_ref[e], preferred_element_type=jnp.float32)
            up_values = jnp.dot(block, up_ref[e], preferred_element_type=jnp.float32)
            act[...] = (jax.nn.silu(gate_values) * up_values).astype(jnp.bfloat16)

        def finish(e):
            for start in range(0, width, chunk):
                rows[place, e, :, start : start + chunk] = jnp.dot(
                    act[...], down_ref[e, :, start : start + chunk], preferred_element_type=jnp.float32
                ).astype(jnp.bfloat16)

        expert(core)
        rows_copy(place).wait()
        finish(core)
        expert(1 - core)
        finish(1 - core)
        part_copy(place).start()

    lag = 2

    @pl.loop(0, n_z + lag)
    def _(step):
        @pl.when(step < n_z)
        def _():
            send_step(step)

        @pl.when(step == 0)
        def _():
            shared_expert()

        @pl.when(step == lag)
        def _():
            for copy in weight_copies:
                copy.wait()

        @pl.when(step >= lag)
        def _():
            compute_step(step - lag)

    def return_step(step):
        place = line_order(z, n_z, n_z - 1 - step)
        part_copy(place).wait_recv()

        @pl.loop(0, n_sp)
        def _(i):
            j = (i + 1) % n_sp
            sp = (me_sp + j) % n_sp
            total = (
                rows[place, core, slot_rows(sp)].astype(jnp.float32)
                + peer_part[place, slot_rows(sp)].astype(jnp.float32)
            ).astype(jnp.bfloat16)

            @pl.when(j > 0)
            def _():
                rows[place, core, slot_rows(sp)] = total
                ret_copy(place, j).start()

            @pl.when(j == 0)
            def _():
                ret[place, slot_rows(me_sp)] = total

    def combine_step(step):
        place = line_order(z, n_z, n_z - 1 - step)

        @pl.loop(1, n_sp)
        def _(j):
            ret_copy(place, j).wait_recv()

        for lane in range(2):
            info = meta_all[2 * place + lane]
            lines = lax.broadcasted_iota(jnp.int32, (all_slots, tokens), 0).astype(jnp.float32)
            picks = jnp.zeros((all_slots, tokens), jnp.float32)
            for choice in range(2):
                ids = info[choice : choice + 1, :tokens]
                spots = spots_all[2 * place + lane, choice : choice + 1, :tokens] + lane * cap
                shard = jnp.floor(ids * 0.5)
                target = jnp.where(
                    ids - 2.0 * shard == core.astype(jnp.float32), shard * slots + spots, -1.0
                )
                picks = picks + jnp.where(
                    lines == target, info[2 + choice : 3 + choice, :tokens], 0.0
                )
            high = picks.astype(jnp.bfloat16)
            low = (picks - high.astype(jnp.float32)).astype(jnp.bfloat16)

            for start in range(0, width, chunk):
                piece = sum(
                    lax.dot_general(
                        part,
                        ret[place, :, start : start + chunk],
                        (((0,), (0,)), ((), ())),
                        preferred_element_type=jnp.float32,
                    )
                    for part in (high, low)
                )

                @pl.when(core == lane)
                def _():
                    own_half[:, start : start + chunk] = piece

                @pl.when(core != lane)
                def _():
                    cross_send[place, :, start : start + chunk] = piece.astype(jnp.bfloat16)

        cross_copy(place).start()
        cross_copy(place).wait_recv()
        own_half[...] = own_half[...] + cross[place].astype(jnp.float32)

        @pl.when(jnp.logical_and(z > 0, place >= z))
        def _():
            pltpu.make_async_copy(hidden_ref, line_in.at[place], line_recv.at[place]).wait()
            own_half[...] = own_half[...] + line_in[place].astype(jnp.float32)

        @pl.when(jnp.logical_and(z < n_z - 1, place <= z))
        def _():
            spot = jnp.where(place == z, n_z, place)
            pltpu.make_async_copy(hidden_ref, line_in.at[spot], line_recv.at[spot]).wait()
            own_half[...] = own_half[...] + line_in[spot].astype(jnp.float32)

        @pl.when(place == z)
        def _():
            values = own_half[...] + result[...]
            center = jnp.mean(values, axis=-1, keepdims=True)
            shifted = values - center
            variance = jnp.mean(shifted * shifted, axis=-1, keepdims=True)
            out_ref[...] = (
                shifted * lax.rsqrt(variance + EPS_LAYER) * norm_gain[...] + norm_bias[...]
            ).astype(jnp.bfloat16)

        @pl.when(place > z)
        def _():
            cross[place] = own_half[...].astype(jnp.bfloat16)
            line_up(place).start()

        @pl.when(place < z)
        def _():
            cross[place] = own_half[...].astype(jnp.bfloat16)
            line_dn(place).start()

    @pl.loop(0, n_z + 1)
    def _(step):
        @pl.when(step < n_z)
        def _():
            return_step(step)

        @pl.when(step > 0)
        def _():
            combine_step(step - 1)

    @pl.loop(0, n_z)
    def _(place):
        pair_copy(hidden_ref, place).wait_send()

        @pl.when(jnp.logical_and(place <= z, z < n_z - 1))
        def _():
            line_copy(hidden_ref, 0, place).wait_send()

        @pl.when(jnp.logical_and(place >= z, z > 0))
        def _():
            line_copy(hidden_ref, 1, place).wait_send()

        part_copy(place).wait_send()
        cross_copy(place).wait_send()

        @pl.when(place != z)
        def _():
            line_up(place).wait_send()

        @pl.loop(1, n_sp)
        def _(j):
            x_copy(place, j).wait_send()
            ret_copy(place, j).wait_send()

    @pl.loop(1, tp_size)
    def _(j):
        meta_copy(j).wait_send()


def moe(hidden, meta, shared, norm, experts, cap):
    expert_gate, expert_up, expert_down = experts
    n_sp = lax.axis_size("sp")
    tp_size = lax.axis_size("tp")
    n_z = tp_size // 2
    tokens, width = hidden.shape
    units = expert_gate.shape[2]
    slots = (2 * cap + 15) // 16 * 16
    all_slots = n_sp * slots
    dma = pltpu.SemaphoreType.DMA
    bf16 = jnp.bfloat16
    return pl.pallas_call(
        functools.partial(moe_kernel, n_sp=n_sp, tp_size=tp_size, cap=cap, slots=slots),
        out_shape=jax.ShapeDtypeStruct((tokens, width), bf16),
        in_specs=[pl.BlockSpec(memory_space=pltpu.VMEM)] * 7
        + [pl.BlockSpec(memory_space=pl.ANY)] * 3,
        out_specs=pl.BlockSpec(memory_space=pltpu.VMEM),
        scratch_shapes=[
            pltpu.VMEM((LOCAL_EXPERTS, width, units), bf16),
            pltpu.VMEM((LOCAL_EXPERTS, width, units), bf16),
            pltpu.VMEM((LOCAL_EXPERTS, units, width), bf16),
            pltpu.VMEM((n_z, 2, tokens, width), bf16),
            pltpu.VMEM((tp_size, 4, 128), jnp.float32),
            pltpu.VMEM((n_z, LOCAL_EXPERTS, all_slots, width), bf16),
            pltpu.VMEM((n_z, all_slots, width), bf16),
            pltpu.VMEM((all_slots, units), bf16),
            pltpu.VMEM((n_z, all_slots, width), bf16),
            pltpu.VMEM((n_z, all_slots, width), bf16),
            pltpu.VMEM((tokens, width), jnp.float32),
            pltpu.VMEM((tokens, width), jnp.float32),
            pltpu.VMEM((tp_size, 2, 128), jnp.float32),
            pltpu.VMEM((n_z, tokens, width), bf16),
            pltpu.VMEM((n_z, tokens, width), bf16),
            pltpu.VMEM((n_z + 1, tokens, width), bf16),
            dma((3,)),
            dma((2, n_z)),
            dma((n_z,)),
            dma((n_z,)),
            dma((n_z,)),
            dma((tp_size,)),
            dma((tp_size,)),
            dma((n_z, n_sp)),
            dma((n_z, n_sp)),
            dma((n_z,)),
            dma((n_z,)),
            dma((n_z,)),
            dma((n_z,)),
            dma((n_z, n_sp)),
            dma((n_z, n_sp)),
            dma((n_z,)),
            dma((n_z,)),
            dma((n_z,)),
            dma((n_z + 1,)),
        ],
        compiler_params=pltpu.CompilerParams(
            has_side_effects=True, vmem_limit_bytes=67_000_000
        ),
    )(hidden, meta, *shared, *[vec.reshape(1, width) for vec in norm], expert_gate, expert_up, expert_down)


def local(
    residual,
    wide_query,
    narrow_query,
    wide_keys,
    narrow_keys,
    wide_values,
    narrow_values,
    wide_query_gain,
    wide_key_gain,
    narrow_query_gain,
    narrow_key_gain,
    wide_out,
    narrow_out,
    first_gain,
    first_bias,
    route_ids,
    route_weights,
    expert_gate,
    expert_up,
    expert_down,
    shared_gate,
    shared_up,
    shared_down,
    second_gain,
    second_bias,
):
    hidden = attention(
        (wide_query, narrow_query),
        (wide_keys, narrow_keys, wide_values, narrow_values),
        (wide_query_gain, wide_key_gain, narrow_query_gain, narrow_key_gain),
        residual,
        wide_out,
        narrow_out,
        first_gain,
        first_bias,
    )
    device_rows = hidden.shape[0]
    sp_size = lax.axis_size("sp")
    top_count = route_ids.shape[1]
    experts = LOCAL_EXPERTS * sp_size
    capacity = max(2, (5 * device_rows * top_count + 4 * experts - 1) // (4 * experts))
    meta = jnp.concatenate([route_ids.astype(jnp.float32), route_weights], axis=1)
    meta = jnp.pad(meta, ((0, 128 - device_rows), (0, 0)), constant_values=-1.0).T
    return moe(
        hidden,
        meta,
        (shared_gate, shared_up, shared_down),
        (second_gain, second_bias),
        (expert_gate, expert_up, expert_down),
        capacity,
    )


def solution(mesh):
    in_specs = (
        P(("sp", "tp"), None),
        P("sp", "tp"),
        P("sp", "tp"),
        P("sp", None),
        P("sp", None),
        P("sp", None),
        P("sp", None),
        P(),
        P(),
        P(),
        P(),
        P("tp", None),
        P("tp", None),
        P(),
        P(),
        P(("sp", "tp"), None),
        P(("sp", "tp"), None),
        P("sp", None, "tp"),
        P("sp", None, "tp"),
        P("sp", "tp", None),
        P(),
        P(),
        P(),
        P(),
        P(),
    )
    out_specs = P(("sp", "tp"), None)
    return jax.shard_map(local, mesh=mesh, in_specs=in_specs, out_specs=out_specs, check_vma=False)
```

```python
import functools
import math

import jax
import jax.numpy as jnp
import numpy as np
from jax import lax
from jax.experimental import pallas as pl
from jax.experimental.pallas import tpu as pltpu
from jax.sharding import PartitionSpec as P

WIDE_HEADS = 16
WIDE_GROUPS = 4
NARROW_HEADS = 32
NARROW_GROUPS = 8
GRID_WIDTH = 64
SEQ_SHARDS = 4
LOCAL_EXPERTS = 2


EPS_HEAD = 1e-06
EPS_LAYER = 1e-05
ALPHA = 2.0**0.25
THETA = 10000.0


def greet(tp_size, sp_peers, me_sp, me_tp):
    barrier = pltpu.get_barrier_semaphore()

    @pl.loop(1, tp_size)
    def _(j):
        pl.semaphore_signal(
            barrier,
            inc=1,
            device_id=(me_sp, (me_tp + j) % tp_size),
            device_id_type=pl.DeviceIdType.MESH,
        )

    for sp in sp_peers:
        pl.semaphore_signal(
            barrier, inc=1, device_id=(sp, me_tp), device_id_type=pl.DeviceIdType.MESH
        )
    return lambda: pl.semaphore_wait(barrier, tp_size - 1 + len(sp_peers))


def line_order(place, count, step):
    mirrored = place >= (count + 1) // 2
    near = jnp.where(mirrored, count - 1 - place, place)
    swing = jnp.where(step % 2 == 1, near + (step + 1) // 2, near - step // 2)
    spot = jnp.where(step <= 2 * near, swing, step)
    return jnp.where(mirrored, count - 1 - spot, spot)


def angle_tables(head_size, lanes, grid_rows):
    half, quarter = head_size // 2, head_size // 4
    lane = np.arange(lanes)
    spot = lane % half
    frequency = THETA ** (-(spot % quarter) / quarter)
    by_row = lane % head_size < half
    sign = np.where(spot < quarter, -1.0, 1.0)
    angles = np.arange(max(grid_rows, GRID_WIDTH))[:, None] * frequency[None, :]
    tables = []
    for keep, count in ((by_row, grid_rows), (~by_row, GRID_WIDTH)):
        tables.append(np.where(keep, np.cos(angles[:count]), 0.0))
        tables.append(np.where(keep, sign * np.sin(angles[:count]), 0.0))
    return [table.astype(np.float32) for table in tables]


def attention_kernel(
    wide_query,
    narrow_query,
    wide_keys,
    narrow_keys,
    wide_values,
    narrow_values,
    wide_query_gain,
    wide_key_gain,
    narrow_query_gain,
    narrow_key_gain,
    wide_row_cos,
    wide_row_sin,
    wide_col_cos,
    wide_col_sin,
    narrow_row_cos,
    narrow_row_sin,
    narrow_col_cos,
    narrow_col_sin,
    residual,
    wide_out,
    narrow_out,
    norm_gain,
    norm_bias,
    hidden_ref,
    wide_kv,
    narrow_kv,
    values_ones,
    wide_heads,
    narrow_heads,
    out_all,
    mixed,
    gathered,
    projected,
    load_sem,
    kv_send,
    kv_recv,
    kv_pair_send,
    kv_pair_recv,
    line_send,
    line_recv,
    out_pair_send,
    out_pair_recv,
    share_send,
    share_recv,
    mixed_send,
    mixed_recv,
    *,
    tp_size,
    shards,
    wide_size,
    narrow_size,
    local_wide,
    local_narrow,
):
    n_z = tp_size // 2
    lanes = 128
    tokens, width = residual.shape
    seg_rows = wide_query.shape[0]
    half_rows = seg_rows // 2
    prep_rows = 256
    prep_grid = prep_rows // GRID_WIDTH
    out_rows = wide_out.shape[0]
    piece = 2 * out_rows // shards
    me_sp = lax.axis_index("sp")
    me_tp = lax.axis_index("tp")
    z = me_tp // 2
    core = me_tp % 2
    peer = me_tp + 1 - 2 * core
    shard = me_sp % shards
    first_sp = me_sp - shard
    kinds = (wide_kv, narrow_kv)

    def remote(src, dst, send_sem, recv_sem, sp, tp):
        return pltpu.make_async_remote_copy(
            src_ref=src,
            dst_ref=dst,
            send_sem=send_sem,
            recv_sem=recv_sem,
            device_id=(sp, tp),
            device_id_type=pl.DeviceIdType.MESH,
        )

    def kv_part(kind, owner, side):
        start = pl.multiple_of(owner * seg_rows + side * half_rows, half_rows)
        return kinds[kind].at[pl.ds(start, half_rows)]

    def kv_copy(kind, j):
        part = kv_part(kind, shard, core)
        return remote(
            part, part, kv_send.at[kind, j], kv_recv.at[kind, j], first_sp + (shard + j) % shards, me_tp
        )

    def kv_pair(kind, j):
        part = kv_part(kind, (shard - j + shards) % shards, core)
        return remote(
            part, part, kv_pair_send.at[kind, j], kv_pair_recv.at[kind, j], me_sp, peer
        )

    def out_piece(place, owner):
        start = (2 * place + core) * 2 * out_rows + owner * piece
        return out_all.at[pl.ds(pl.multiple_of(start, piece), piece)]

    def line_copy(place, way):
        part = out_piece(place, shard)
        return remote(
            part, part, line_send.at[way, place], line_recv.at[place], me_sp, me_tp + 2 - 4 * way
        )

    def passes(place, way):
        if way == 0:
            return jnp.logical_and(place <= z, z < n_z - 1)
        return jnp.logical_and(place >= z, z > 0)

    def out_pair(place, j):
        part = out_piece(place, (shard - j + shards) % shards)
        return remote(part, part, out_pair_send.at[place, j], out_pair_recv.at[place, j], me_sp, peer)

    def own_pair():
        part = out_all.at[pl.ds(pl.multiple_of(me_tp * 2 * out_rows, 2 * out_rows), 2 * out_rows)]
        return remote(part, part, out_pair_send.at[z, 0], out_pair_recv.at[z, 0], me_sp, peer)

    def share_copy(place, j):
        part = out_piece(place, shard)
        return remote(
            part, part, share_send.at[place, j], share_recv.at[place, j],
            first_sp + (shard + j) % shards, me_tp,
        )

    def mixed_copy(kind, b):
        target = (me_tp + 1 + b) % tp_size
        return remote(
            mixed.at[kind, target],
            gathered.at[:, pl.ds(pl.multiple_of((2 * me_tp + kind) * lanes, lanes), lanes)],
            mixed_send.at[kind, b],
            mixed_recv.at[kind, b],
            me_sp,
            target,
        )

    loads = [
        pltpu.make_async_copy(
            src,
            out_all.at[pl.ds(pl.multiple_of((2 * me_tp + i) * out_rows, out_rows), out_rows)],
            load_sem.at[i],
        )
        for i, src in enumerate((wide_out, narrow_out))
    ]
    await_peers = greet(
        tp_size, [first_sp + (shard + j) % shards for j in range(1, shards)], me_sp, me_tp
    )
    for copy in loads:
        copy.start()

    lane = lax.broadcasted_iota(jnp.int32, (1, lanes), 1)

    def spread_gain(gain):
        size = gain.shape[1]
        row = lax.broadcasted_iota(jnp.int32, (size, lanes), 0)
        column = lax.broadcasted_iota(jnp.int32, (size, lanes), 1)
        return jnp.dot(
            jnp.broadcast_to(gain[...], (8, size)),
            jnp.where(column % size == row, 1.0, 0.0),
            precision=lax.Precision.HIGHEST,
            preferred_element_type=jnp.float32,
        )[0:1]

    gains = [
        spread_gain(gain)
        for gain in (wide_query_gain, wide_key_gain, narrow_query_gain, narrow_key_gain)
    ]

    def normalized(values, size, gain_row, row_cos, row_sin, col_cos, col_sin, i):
        squares = values * values
        high = squares.astype(jnp.bfloat16)
        low = (squares - high.astype(jnp.float32)).astype(jnp.bfloat16)
        left = lax.broadcasted_iota(jnp.int32, (lanes, lanes), 0) // size
        right = lax.broadcasted_iota(jnp.int32, (lanes, lanes), 1) // size
        same = jnp.where(left == right, 1.0, 0.0).astype(jnp.bfloat16)
        total = jnp.dot(high, same, preferred_element_type=jnp.float32) + jnp.dot(
            low, same, preferred_element_type=jnp.float32
        )
        scaled = values * lax.rsqrt(total * (1.0 / size) + EPS_HEAD) * gains[gain_row]
        quarter = size // 4
        partner = jnp.where(
            lane % (size // 2) < quarter,
            pltpu.roll(scaled, lanes - quarter, 1),
            pltpu.roll(scaled, quarter, 1),
        )
        grid_row = (shard * (seg_rows // prep_rows) + i) * prep_grid

        def spread(by_row, by_col):
            lines = by_row[pl.ds(grid_row, prep_grid), :]
            return jnp.concatenate([lines[g : g + 1, :] + by_col[...] for g in range(prep_grid)], axis=0)

        return scaled * spread(row_cos, col_cos) + partner * spread(row_sin, col_sin)

    wide_tables = (wide_row_cos, wide_row_sin, wide_col_cos, wide_col_sin)
    narrow_tables = (narrow_row_cos, narrow_row_sin, narrow_col_cos, narrow_col_sin)

    def column_pick(source, group, size):
        column = lax.broadcasted_iota(jnp.int32, (source.shape[1], lanes), 0)
        return jnp.where(column == group * size + lane % size, 1.0, 0.0).astype(jnp.bfloat16)

    def key_step(kind, i, keys, values, picks, size, gain_row, tables):
        rows = pl.ds(pl.multiple_of(i * prep_rows, prep_rows), prep_rows)
        own_keys = jnp.dot(keys[rows, :], picks, preferred_element_type=jnp.float32)
        own_values = jnp.dot(values[rows, :], picks, preferred_element_type=jnp.float32)
        rotated = normalized(own_keys, size, gain_row, *tables, i)
        packed = jnp.where((lane // size) % 2 == 0, rotated, own_values).astype(jnp.bfloat16)
        start = pl.multiple_of(shard * seg_rows + i * prep_rows, prep_rows)
        kinds[kind][pl.ds(start, prep_rows), :] = packed

    per_wide = WIDE_HEADS // WIDE_GROUPS
    per_narrow = NARROW_HEADS // NARROW_GROUPS
    wide_picks = column_pick(wide_keys, me_tp * local_wide // per_wide, wide_size)
    lower_group = 2 * z * local_narrow // per_narrow
    upper_group = (2 * z + 1) * local_narrow // per_narrow
    narrow_picks = column_pick(
        narrow_keys, jnp.where(lane < lanes // 2, lower_group, upper_group), narrow_size
    )
    blocks = seg_rows // prep_rows

    @pl.loop(0, blocks)
    def _(i):
        key_step(0, i, wide_keys, wide_values, wide_picks, wide_size, 1, wide_tables)

    await_peers()
    for j in range(1, shards):
        kv_copy(0, j).start()

    for copy in loads:
        copy.wait()
    own_pair().start()

    for way in range(2):

        @pl.when(passes(z, way))
        def _():
            line_copy(z, way).start()

    @pl.loop(0, blocks)
    def _(i):
        key_step(1, i, narrow_keys, narrow_values, narrow_picks, narrow_size, 3, narrow_tables)

    for j in range(1, shards):
        kv_copy(1, j).start()
    @pl.loop(0, blocks)
    def _(i):
        rows = pl.ds(pl.multiple_of(i * prep_rows, prep_rows), prep_rows)
        rotated = normalized(
            wide_query[rows, :].astype(jnp.float32), wide_size, 0, *wide_tables, i
        )
        for h in range(local_wide):
            moved = rotated if h == 0 else pltpu.roll(rotated, lanes - h * wide_size, 1)
            wide_heads[h, rows] = jnp.where(lane < wide_size, moved, 0.0).astype(jnp.bfloat16)
        rotated = normalized(
            narrow_query[rows, :].astype(jnp.float32), narrow_size, 2, *narrow_tables, i
        )
        for h in range(local_narrow):
            shift = (core * (lanes // 2) + lanes - h * narrow_size) % lanes
            moved = pltpu.roll(rotated, shift, 1)
            kept = lane // narrow_size == 2 * core
            narrow_heads[h, rows] = jnp.where(kept, moved, 0.0).astype(jnp.bfloat16)

    def attend(block, kv, size):
        scores = lax.dot_general(
            block, kv[...], (((1,), (1,)), ((), ())), preferred_element_type=jnp.float32
        )
        largest = jnp.max(scores, axis=-1, keepdims=True)
        factor = math.log2(math.e) * size ** (-0.5)
        weights = jnp.exp2((scores - largest) * factor).astype(jnp.bfloat16)
        sums = jnp.dot(weights, values_ones[...], preferred_element_type=jnp.float32)
        return sums / sums[:, 0:1]

    def relay_kv(kind):
        for j in range(1, shards):
            kv_copy(kind, j).wait_recv()
            kv_pair(kind, j).start()
        for j in range(1, shards):
            kv_pair(kind, j).wait_recv()
        size = (wide_size, narrow_size)[kind]
        keep = jnp.where((lane // size) % 2 == 1, 1.0, 0.0).astype(jnp.bfloat16)
        fill = jnp.where((lane // size) % 2 == 1, 0.0, 1.0).astype(jnp.bfloat16)

        @pl.loop(0, shards * blocks)
        def _(i):
            rows = pl.ds(pl.multiple_of(i * prep_rows, prep_rows), prep_rows)
            values_ones[rows, :] = kinds[kind][rows, :] * keep + fill

    def put_mixed(kind, b, target, value):
        @pl.when(b < tp_size - 1)
        def _():
            mixed[kind, target] = value
            mixed_copy(kind, b).start()

        @pl.when(b == tp_size - 1)
        def _():
            spot = pl.multiple_of((2 * target + kind) * lanes, lanes)
            gathered[:, pl.ds(spot, lanes)] = value

    def line_wait(place):
        part = out_piece(place, shard)
        pltpu.make_async_copy(part, part, line_recv.at[place]).wait()

    def forward_step(step):
        place = line_order(z, n_z, step)
        for way in range(2):

            @pl.when(passes(place, way))
            def _():
                line_wait(place)
                line_copy(place, way).start()

    def share_step(step):
        place = line_order(z, n_z, step)

        @pl.when(jnp.logical_not(jnp.logical_or(passes(place, 0), passes(place, 1))))
        def _():
            line_wait(place)

        for j in range(1, shards):
            share_copy(place, j).start()
        out_pair(place, 0).start()

    relay_kv(0)
    for step in range(1, min(3, n_z)):
        forward_step(step)

    @pl.loop(0, tp_size)
    def _(b):
        @pl.when(jnp.logical_and(b >= n_z, b < 2 * n_z - 3))
        def _():
            forward_step(b - n_z + 3)

        @pl.when(jnp.logical_or(b == n_z // 2, b == n_z + n_z // 2))
        def _():
            share_step(b // n_z + 1)

        target = (me_tp + 1 + b) % tp_size
        rows = pl.ds(pl.multiple_of(target * tokens, tokens), tokens)
        block = jnp.concatenate([wide_heads[h, rows] for h in range(local_wide)], axis=0)
        values = attend(block, wide_kv, wide_size)
        total = jnp.zeros((tokens, lanes), jnp.float32)
        for h in range(local_wide):
            part = values[h * tokens : (h + 1) * tokens]
            shift = ((h + 1) * wide_size) % lanes
            moved = part if shift == 0 else pltpu.roll(part, shift, 1)
            total = total + jnp.where(lane // wide_size == h, moved, 0.0)
        put_mixed(0, b, target, total.astype(jnp.bfloat16))

    relay_kv(1)

    @pl.loop(0, tp_size)
    def _(b):
        @pl.when(jnp.logical_and(b > 0, b + 2 < n_z))
        def _():
            share_step(b + 2)

        @pl.when(b > tp_size - n_z)
        def _():
            place = line_order(z, n_z, b - (tp_size - n_z))
            for j in range(1, shards):
                share_copy(place, j).wait_recv()
                out_pair(place, j).start()

        target = (me_tp + 1 + b) % tp_size
        rows = pl.ds(pl.multiple_of(target * tokens, tokens), tokens)
        total = jnp.zeros((tokens, lanes), jnp.float32)
        for first in range(0, local_narrow, 2):
            block = jnp.concatenate([narrow_heads[first + h, rows] for h in range(2)], axis=0)
            values = attend(block, narrow_kv, narrow_size)
            for h in range(2):
                part = values[h * tokens : (h + 1) * tokens]
                shift = (
                    (first + h) * narrow_size + 2 * lanes - core * (lanes // 2) - narrow_size
                ) % lanes
                moved = pltpu.roll(part, shift, 1)
                total = total + jnp.where(lane // narrow_size == first + h, moved, 0.0)
        put_mixed(1, b, target, total.astype(jnp.bfloat16))

    @pl.loop(0, n_z)
    def _(place):
        @pl.when(place == z)
        def _():
            own_pair().wait_recv()

        @pl.when(place != z)
        def _():
            for j in range(shards):
                out_pair(place, j).wait_recv()

    @pl.loop(0, tp_size - 1)
    def _(b):
        mixed_copy(0, b).wait_recv()
        mixed_copy(1, b).wait_recv()

    chunk = 512
    for start in range(0, width, chunk):

        total = ALPHA * residual[:, start : start + chunk].astype(jnp.float32)
        if out_rows == lanes:
            total = total + jnp.dot(
                gathered[...], out_all[:, start : start + chunk], preferred_element_type=jnp.float32
            )
        else:
            for q in range(2 * tp_size):
                total = total + jnp.dot(
                    gathered[:, q * lanes : q * lanes + out_rows],
                    out_all[q * out_rows : (q + 1) * out_rows, start : start + chunk],
                    preferred_element_type=jnp.float32,
                )
        projected[:, start : start + chunk] = total

    values = projected[...]
    center = jnp.mean(values, axis=-1, keepdims=True)
    shifted = values - center
    variance = jnp.mean(shifted * shifted, axis=-1, keepdims=True)
    hidden_ref[...] = (
        shifted * lax.rsqrt(variance + EPS_LAYER) * norm_gain[...] + norm_bias[...]
    ).astype(jnp.bfloat16)

    own_pair().wait_send()
    for j in range(1, shards):
        for kind in range(2):
            kv_copy(kind, j).wait_send()
            kv_pair(kind, j).wait_send()

    @pl.loop(0, n_z)
    def _(place):
        for way in range(2):

            @pl.when(passes(place, way))
            def _():
                line_copy(place, way).wait_send()

        @pl.when(place != z)
        def _():
            for j in range(shards):
                out_pair(place, j).wait_send()
            for j in range(1, shards):
                share_copy(place, j).wait_send()

    @pl.loop(0, tp_size - 1)
    def _(b):
        mixed_copy(0, b).wait_send()
        mixed_copy(1, b).wait_send()


def attention(
    queries, keys_values, gain_vecs, residual, wide_out, narrow_out, first_gain, first_bias
):
    tp_size = lax.axis_size("tp")
    n_z = tp_size // 2
    lanes = 128
    tokens, width = residual.shape
    seg_rows = queries[0].shape[0]
    shards = SEQ_SHARDS
    sizes = gain_vecs[0].shape[0], gain_vecs[2].shape[0]
    local_heads = [q.shape[1] // size for q, size in zip(queries, sizes)]
    queries = [jnp.pad(q, ((0, 0), (0, lanes - q.shape[1]))) for q in queries]
    gains = [gain.reshape(1, -1) for gain in gain_vecs]
    grid_rows = shards * seg_rows // GRID_WIDTH
    tables = [
        jnp.asarray(table)
        for size in sizes
        for table in angle_tables(size, lanes, grid_rows)
    ]
    bf16 = jnp.bfloat16
    dma = pltpu.SemaphoreType.DMA
    vmem = pl.BlockSpec(memory_space=pltpu.VMEM)
    hbm = pl.BlockSpec(memory_space=pl.ANY)
    return pl.pallas_call(
        functools.partial(
            attention_kernel,
            tp_size=tp_size,
            shards=shards,
            wide_size=sizes[0],
            narrow_size=sizes[1],
            local_wide=local_heads[0],
            local_narrow=local_heads[1],
        ),
        out_shape=jax.ShapeDtypeStruct((tokens, width), bf16),
        in_specs=[vmem] * 19 + [hbm] * 2 + [vmem] * 2,
        out_specs=vmem,
        scratch_shapes=[
            pltpu.VMEM((shards * seg_rows, lanes), bf16),
            pltpu.VMEM((shards * seg_rows, lanes), bf16),
            pltpu.VMEM((shards * seg_rows, lanes), bf16),
            pltpu.VMEM((local_heads[0], seg_rows, lanes), bf16),
            pltpu.VMEM((local_heads[1], seg_rows, lanes), bf16),
            pltpu.VMEM((2 * tp_size * wide_out.shape[0], width), bf16),
            pltpu.VMEM((2, tp_size, tokens, lanes), bf16),
            pltpu.VMEM((tokens, 2 * tp_size * lanes), bf16),
            pltpu.VMEM((tokens, width), jnp.float32),
            dma((2,)),
            dma((2, shards)),
            dma((2, shards)),
            dma((2, shards)),
            dma((2, shards)),
            dma((2, n_z)),
            dma((n_z,)),
            dma((n_z, shards)),
            dma((n_z, shards)),
            dma((n_z, shards)),
            dma((n_z, shards)),
            dma((2, tp_size)),
            dma((2, tp_size)),
        ],
        compiler_params=pltpu.CompilerParams(
            collective_id=0, has_side_effects=True, vmem_limit_bytes=66_000_000
        ),
    )(
        *queries,
        *keys_values,
        *gains,
        *tables,
        residual,
        wide_out,
        narrow_out,
        first_gain.reshape(1, width),
        first_bias.reshape(1, width),
    )


def moe_kernel(
    hidden_ref,
    meta_ref,
    norm_gain,
    norm_bias,
    shared_gate_hbm,
    shared_up_hbm,
    shared_down_hbm,
    gate_hbm,
    up_hbm,
    down_hbm,
    out_ref,
    gate_ref,
    up_ref,
    down_ref,
    shared_gate,
    shared_up,
    shared_down,
    hid,
    meta_all,
    rows,
    stage,
    act,
    peer_part,
    ret,
    own_half,
    result,
    spots_all,
    cross_send,
    cross,
    line_in,
    far_in,
    far_line_in,
    far_sum,
    weight_sem,
    z_send,
    z_recv,
    pair_send,
    pair_recv,
    meta_send,
    meta_recv,
    x_send,
    x_recv,
    rows_send,
    rows_recv,
    part_send,
    part_recv,
    ret_send,
    ret_recv,
    cross_send_sem,
    cross_recv,
    line_send,
    line_recv,
    far_send_sem,
    far_line_send,
    far_line_recv,
    *,
    n_sp,
    tp_size,
    cap,
    slots,
    by_line,
):
    n_z = tp_size // 2
    tokens, width = hidden_ref.shape
    all_slots = n_sp * slots
    chunk = 512
    lag = 2
    expert_lines = (LOCAL_EXPERTS * n_sp + 15) // 16 * 16
    me_sp = lax.axis_index("sp")
    me_tp = lax.axis_index("tp")
    z = me_tp // 2
    core = me_tp % 2
    peer = me_tp + 1 - 2 * core
    far_sp = n_sp - 1 - me_sp
    far_send = (2 * n_sp - 1 - 2 * me_sp) % n_sp
    far_recv = (2 * me_sp + 1) % n_sp
    relays = core == 1 if by_line else False

    def skipped(j, far_j, place):
        if not by_line:
            return j < 0
        return jnp.logical_and(core == 1, jnp.logical_and(j == far_j, place != z))

    def is_far(j, far_j):
        if not by_line:
            return j < 0
        return jnp.logical_and(core == 1, j == far_j)

    def remote(src, dst, send_sem, recv_sem, sp, tp):
        return pltpu.make_async_remote_copy(
            src_ref=src,
            dst_ref=dst,
            send_sem=send_sem,
            recv_sem=recv_sem,
            device_id=(sp, tp),
            device_id_type=pl.DeviceIdType.MESH,
        )

    weight_copies = [
        pltpu.make_async_copy(src, dst, weight_sem.at[i])
        for i, (src, dst) in enumerate(
            (
                (shared_gate_hbm, shared_gate),
                (shared_up_hbm, shared_up),
                (shared_down_hbm, shared_down),
                (gate_hbm, gate_ref),
                (up_hbm, up_ref),
                (down_hbm, down_ref),
            )
        )
    ]

    def line_copy(src, way, place):
        return remote(
            src,
            hid.at[place, core],
            z_send.at[way, place],
            z_recv.at[place],
            me_sp,
            me_tp + 2 - 4 * way,
        )

    def pair_copy(src, place):
        return remote(
            src, hid.at[place, core], pair_send.at[place], pair_recv.at[place], me_sp, peer
        )

    def meta_copy(j):
        return remote(
            meta_ref,
            meta_all.at[me_tp],
            meta_send.at[j],
            meta_recv.at[j],
            me_sp,
            (me_tp + j) % tp_size,
        )

    def slot_rows(sp):
        return pl.ds(pl.multiple_of(sp * slots, slots), slots)

    def x_copy(place, j):
        sp = (me_sp + j) % n_sp
        return remote(
            stage.at[place, slot_rows(sp)],
            rows.at[place, core, slot_rows(me_sp)],
            x_send.at[place, j],
            x_recv.at[place, j],
            sp,
            me_tp,
        )

    def far_copy(place):
        return remote(
            stage.at[place, slot_rows(far_sp)],
            far_in.at[place],
            x_send.at[place, far_send],
            x_recv.at[place, far_send],
            far_sp,
            me_tp,
        )

    def far_relay(place, way):
        return remote(
            far_in.at[place],
            far_in.at[place],
            far_send_sem.at[way, place],
            x_recv.at[place, far_recv],
            me_sp,
            me_tp + 2 - 4 * way,
        )

    def far_line(place, way):
        spot = place if way == 0 else jnp.where(place == z - 1, n_z, place)
        return remote(
            rows.at[place, core, slot_rows(far_sp)],
            far_line_in.at[spot],
            far_line_send.at[place],
            far_line_recv.at[spot],
            me_sp,
            me_tp + 2 - 4 * way,
        )

    def passes(place, way):
        if way == 0:
            return jnp.logical_and(place <= z, z < n_z - 1)
        return jnp.logical_and(place >= z, z > 0)

    def rows_copy(place):
        return remote(
            rows.at[place, core],
            rows.at[place, core],
            rows_send.at[place],
            rows_recv.at[place],
            me_sp,
            peer,
        )

    def part_copy(place):
        return remote(
            rows.at[place, 1 - core],
            peer_part.at[place],
            part_send.at[place],
            part_recv.at[place],
            me_sp,
            peer,
        )

    def ret_copy(place, j):
        sp = (me_sp + j) % n_sp
        return remote(
            rows.at[place, core, slot_rows(sp)],
            ret.at[place, slot_rows(me_sp)],
            ret_send.at[place, j],
            ret_recv.at[place, j],
            sp,
            me_tp,
        )

    def cross_copy(place):
        return remote(
            cross_send.at[place],
            cross.at[place],
            cross_send_sem.at[place],
            cross_recv.at[place],
            me_sp,
            peer,
        )

    def line_up(place):
        return remote(
            cross.at[place], line_in.at[place], line_send.at[place], line_recv.at[place], me_sp, me_tp + 2
        )

    def line_dn(place):
        spot = jnp.where(place == z - 1, n_z, place)
        return remote(
            cross.at[place], line_in.at[spot], line_send.at[place], line_recv.at[spot], me_sp, me_tp - 2
        )

    await_peers = greet(
        tp_size, [(me_sp + j) % n_sp for j in range(1, n_sp)], me_sp, me_tp
    )
    for copy in weight_copies:
        copy.start()
    hid[z, core] = hidden_ref[...]
    meta_all[me_tp] = meta_ref[...]
    await_peers()
    pair_copy(hidden_ref, z).start()

    @pl.when(z < n_z - 1)
    def _():
        line_copy(hidden_ref, 0, z).start()

    @pl.when(z > 0)
    def _():
        line_copy(hidden_ref, 1, z).start()

    @pl.loop(1, tp_size)
    def _(j):
        meta_copy(j).start()

    def selection(place, sp, weighted):
        expert = (LOCAL_EXPERTS * sp + core).astype(jnp.float32)
        parts = []
        for lane in range(2):
            info = meta_all[2 * place + lane]
            line = lax.broadcasted_iota(jnp.int32, (slots, tokens), 0).astype(jnp.float32)
            part = jnp.zeros((slots, tokens), jnp.float32)
            for choice in range(2):
                ids = info[choice : choice + 1, :tokens]
                spots = spots_all[2 * place + lane, choice : choice + 1, :tokens] + lane * cap
                target = jnp.where(ids == expert, spots, -1.0)
                value = info[2 + choice : 3 + choice, :tokens] if weighted else 1.0
                part = part + jnp.where(line == target, value, 0.0)
            parts.append(part)
        return jnp.concatenate(parts, axis=1)

    def clear_far():
        if by_line:

            @pl.when(core == 1)
            def _():
                @pl.loop(0, n_z)
                def _(place):
                    @pl.when(place != z)
                    def _():
                        ret[place, slot_rows(far_sp)] = jnp.zeros((slots, width), jnp.bfloat16)

    def shared_expert():
        for copy in weight_copies[:3]:
            copy.wait()
        gate_values = jnp.dot(hidden_ref[...], shared_gate[...], preferred_element_type=jnp.float32)
        up_values = jnp.dot(hidden_ref[...], shared_up[...], preferred_element_type=jnp.float32)
        active = (jax.nn.silu(gate_values) * up_values).astype(jnp.bfloat16)
        for start in range(0, width, chunk):
            cols = slice(start, start + chunk)
            result[:, cols] = ALPHA * hidden_ref[:, cols].astype(jnp.float32) + jnp.dot(
                active, shared_down[:, cols], preferred_element_type=jnp.float32
            )

    def send_step(step):
        place = line_order(z, n_z, step)

        @pl.when(step > 0)
        def _():
            pltpu.make_async_copy(hidden_ref, hid.at[place, core], z_recv.at[place]).wait()

            @pl.when(jnp.logical_and(place < z, z < n_z - 1))
            def _():
                line_copy(hid.at[place, core], 0, place).start()

            @pl.when(jnp.logical_and(place > z, z > 0))
            def _():
                line_copy(hid.at[place, core], 1, place).start()

            pair_copy(hid.at[place, core], place).start()

        pltpu.make_async_copy(hidden_ref, hid.at[place, 1 - core], pair_recv.at[place]).wait()
        for lane in range(2):
            j = (me_tp - 2 * place - lane + tp_size) % tp_size

            @pl.when(j > 0)
            def _():
                pltpu.make_async_copy(meta_ref, meta_all.at[2 * place + lane], meta_recv.at[j]).wait()

            info = meta_all[2 * place + lane]
            line = lax.broadcasted_iota(jnp.int32, (expert_lines, 128), 0).astype(jnp.float32)
            first = jnp.where(line == info[0:1, :], 1.0, 0.0)
            second = jnp.where(line == info[1:2, :], 1.0, 0.0)
            before = lax.broadcasted_iota(jnp.int32, (128, 128), 0) < lax.broadcasted_iota(
                jnp.int32, (128, 128), 1
            )
            counts = jnp.dot(
                (first + second).astype(jnp.bfloat16),
                jnp.where(before, 1.0, 0.0).astype(jnp.bfloat16),
                preferred_element_type=jnp.float32,
            )
            spots_all[2 * place + lane, 0:1] = jnp.sum(first * counts, axis=0, keepdims=True)
            spots_all[2 * place + lane, 1:2] = jnp.sum(second * counts, axis=0, keepdims=True)

        @pl.loop(0, n_sp)
        def _(i):
            j = (i + 1) % n_sp
            sp = (me_sp + j) % n_sp

            @pl.when(jnp.logical_not(skipped(j, far_send, place)))
            def _():
                picks = selection(place, sp, False).astype(jnp.bfloat16)
                for start in range(0, width, chunk):
                    piece = (
                        jnp.dot(
                            picks[:, :tokens],
                            hid[place, 0, :, start : start + chunk],
                            preferred_element_type=jnp.float32,
                        )
                        + jnp.dot(
                            picks[:, tokens:],
                            hid[place, 1, :, start : start + chunk],
                            preferred_element_type=jnp.float32,
                        )
                    ).astype(jnp.bfloat16)
                    stage[place, slot_rows(sp), start : start + chunk] = piece

                @pl.when(jnp.logical_and(j > 0, jnp.logical_not(is_far(j, far_send))))
                def _():
                    x_copy(place, j).start()

                if by_line:

                    @pl.when(is_far(j, far_send))
                    def _():
                        far_copy(place).start()

            @pl.when(j == 0)
            def _():
                rows[place, core, slot_rows(me_sp)] = stage[place, slot_rows(me_sp)]

    def compute_step(step):
        place = line_order(z, n_z, step)

        if by_line:

            def start_relay(place):
                for way in range(2):

                    @pl.when(passes(place, way))
                    def _():
                        far_relay(place, way).start()

            @pl.when(relays)
            def _():
                @pl.when(step == n_z - 1 - lag)
                def _():
                    for earlier in range(n_z - 1 - lag):
                        start_relay(line_order(z, n_z, earlier))

                far_relay(place, 0).wait_recv()

                @pl.when(step >= n_z - 1 - lag)
                def _():
                    start_relay(place)

                rows[place, core, slot_rows(far_sp)] = far_in[place]

        @pl.loop(1, n_sp)
        def _(j):
            @pl.when(jnp.logical_not(is_far(j, far_recv)))
            def _():
                x_copy(place, j).wait_recv()

        rows_copy(place).start()

        def expert(e):
            block = rows[place, e]
            gate_values = jnp.dot(block, gate_ref[e], preferred_element_type=jnp.float32)
            up_values = jnp.dot(block, up_ref[e], preferred_element_type=jnp.float32)
            act[...] = (jax.nn.silu(gate_values) * up_values).astype(jnp.bfloat16)

        def finish(e):
            for start in range(0, width, chunk):
                rows[place, e, :, start : start + chunk] = jnp.dot(
                    act[...], down_ref[e, :, start : start + chunk], preferred_element_type=jnp.float32
                ).astype(jnp.bfloat16)

        expert(core)
        rows_copy(place).wait_send()
        finish(core)
        rows_copy(place).wait_recv()
        expert(1 - core)
        finish(1 - core)
        part_copy(place).start()

    @pl.loop(0, n_z + lag)
    def _(step):
        @pl.when(step < n_z)
        def _():
            send_step(step)

        @pl.when(step == 0)
        def _():
            if by_line:
                clear_far()
            shared_expert()

        @pl.when(step == lag)
        def _():
            for copy in weight_copies[3:]:
                copy.wait()

        @pl.when(step >= lag)
        def _():
            compute_step(step - lag)

    def return_step(step):
        place = line_order(z, n_z, n_z - 1 - step)
        part_copy(place).wait_recv()

        @pl.loop(0, n_sp)
        def _(i):
            j = (i + 1) % n_sp
            sp = (me_sp + j) % n_sp

            @pl.when(jnp.logical_not(is_far(j, far_send)))
            def _():
                total = (
                    rows[place, core, slot_rows(sp)].astype(jnp.float32)
                    + peer_part[place, slot_rows(sp)].astype(jnp.float32)
                ).astype(jnp.bfloat16)

                @pl.when(j > 0)
                def _():
                    rows[place, core, slot_rows(sp)] = total
                    ret_copy(place, j).start()

                @pl.when(j == 0)
                def _():
                    ret[place, slot_rows(me_sp)] = total

        if by_line:

            @pl.when(relays)
            def _():
                far_sum[...] = rows[place, core, slot_rows(far_sp)].astype(jnp.float32) + peer_part[
                    place, slot_rows(far_sp)
                ].astype(jnp.float32)

                @pl.when(jnp.logical_and(z > 0, place >= z))
                def _():
                    pltpu.make_async_copy(
                        far_in.at[place], far_line_in.at[place], far_line_recv.at[place]
                    ).wait()
                    far_sum[...] = far_sum[...] + far_line_in[place].astype(jnp.float32)

                @pl.when(jnp.logical_and(z < n_z - 1, place <= z))
                def _():
                    spot = jnp.where(place == z, n_z, place)
                    pltpu.make_async_copy(
                        far_in.at[place], far_line_in.at[spot], far_line_recv.at[spot]
                    ).wait()
                    far_sum[...] = far_sum[...] + far_line_in[spot].astype(jnp.float32)

                rows[place, core, slot_rows(far_sp)] = far_sum[...].astype(jnp.bfloat16)

                @pl.when(place == z)
                def _():
                    ret_copy(place, far_send).start()

                @pl.when(place > z)
                def _():
                    far_line(place, 0).start()

                @pl.when(place < z)
                def _():
                    far_line(place, 1).start()

    def combine_step(step):
        place = line_order(z, n_z, n_z - 1 - step)

        @pl.loop(1, n_sp)
        def _(j):
            @pl.when(jnp.logical_not(skipped(j, far_recv, place)))
            def _():
                ret_copy(place, j).wait_recv()

        for lane in range(2):
            info = meta_all[2 * place + lane]
            lines = lax.broadcasted_iota(jnp.int32, (all_slots, tokens), 0).astype(jnp.float32)
            picks = jnp.zeros((all_slots, tokens), jnp.float32)
            for choice in range(2):
                ids = info[choice : choice + 1, :tokens]
                spots = spots_all[2 * place + lane, choice : choice + 1, :tokens] + lane * cap
                shard = jnp.floor(ids * 0.5)
                target = jnp.where(
                    ids - 2.0 * shard == core.astype(jnp.float32), shard * slots + spots, -1.0
                )
                picks = picks + jnp.where(
                    lines == target, info[2 + choice : 3 + choice, :tokens], 0.0
                )
            high = picks.astype(jnp.bfloat16)
            low = (picks - high.astype(jnp.float32)).astype(jnp.bfloat16)

            for start in range(0, width, chunk):
                piece = sum(
                    lax.dot_general(
                        part,
                        ret[place, :, start : start + chunk],
                        (((0,), (0,)), ((), ())),
                        preferred_element_type=jnp.float32,
                    )
                    for part in (high, low)
                )

                @pl.when(core == lane)
                def _():
                    own_half[:, start : start + chunk] = piece

                @pl.when(core != lane)
                def _():
                    cross_send[place, :, start : start + chunk] = piece.astype(jnp.bfloat16)

        cross_copy(place).start()
        cross_copy(place).wait_recv()
        own_half[...] = own_half[...] + cross[place].astype(jnp.float32)

        @pl.when(jnp.logical_and(z > 0, place >= z))
        def _():
            pltpu.make_async_copy(hidden_ref, line_in.at[place], line_recv.at[place]).wait()
            own_half[...] = own_half[...] + line_in[place].astype(jnp.float32)

        @pl.when(jnp.logical_and(z < n_z - 1, place <= z))
        def _():
            spot = jnp.where(place == z, n_z, place)
            pltpu.make_async_copy(hidden_ref, line_in.at[spot], line_recv.at[spot]).wait()
            own_half[...] = own_half[...] + line_in[spot].astype(jnp.float32)

        @pl.when(place == z)
        def _():
            values = own_half[...] + result[...]
            center = jnp.mean(values, axis=-1, keepdims=True)
            shifted = values - center
            variance = jnp.mean(shifted * shifted, axis=-1, keepdims=True)
            out_ref[...] = (
                shifted * lax.rsqrt(variance + EPS_LAYER) * norm_gain[...] + norm_bias[...]
            ).astype(jnp.bfloat16)

        @pl.when(place > z)
        def _():
            cross[place] = own_half[...].astype(jnp.bfloat16)
            line_up(place).start()

        @pl.when(place < z)
        def _():
            cross[place] = own_half[...].astype(jnp.bfloat16)
            line_dn(place).start()

    @pl.loop(0, n_z + 1)
    def _(step):
        @pl.when(step < n_z)
        def _():
            return_step(step)

        @pl.when(step > 0)
        def _():
            combine_step(step - 1)

    @pl.loop(0, n_z)
    def _(place):
        pair_copy(hidden_ref, place).wait_send()

        @pl.when(jnp.logical_and(place <= z, z < n_z - 1))
        def _():
            line_copy(hidden_ref, 0, place).wait_send()

        @pl.when(jnp.logical_and(place >= z, z > 0))
        def _():
            line_copy(hidden_ref, 1, place).wait_send()

        part_copy(place).wait_send()
        cross_copy(place).wait_send()

        @pl.when(place != z)
        def _():
            line_up(place).wait_send()

        @pl.loop(1, n_sp)
        def _(j):
            @pl.when(jnp.logical_not(skipped(j, far_send, place)))
            def _():
                x_copy(place, j).wait_send()
                ret_copy(place, j).wait_send()

        if by_line:

            @pl.when(relays)
            def _():
                for way in range(2):

                    @pl.when(passes(place, way))
                    def _():
                        far_relay(place, way).wait_send()

                @pl.when(place != z)
                def _():
                    far_line(place, 0).wait_send()

    @pl.loop(1, tp_size)
    def _(j):
        meta_copy(j).wait_send()


def moe(hidden, meta, shared, norm, experts, cap):
    expert_gate, expert_up, expert_down = experts
    n_sp = lax.axis_size("sp")
    tp_size = lax.axis_size("tp")
    n_z = tp_size // 2
    tokens, width = hidden.shape
    units = expert_gate.shape[2]
    slots = (2 * cap + 15) // 16 * 16
    all_slots = n_sp * slots
    by_line = n_sp == 4
    dma = pltpu.SemaphoreType.DMA
    bf16 = jnp.bfloat16
    return pl.pallas_call(
        functools.partial(
            moe_kernel, n_sp=n_sp, tp_size=tp_size, cap=cap, slots=slots, by_line=by_line
        ),
        out_shape=jax.ShapeDtypeStruct((tokens, width), bf16),
        in_specs=[pl.BlockSpec(memory_space=pltpu.VMEM)] * 4
        + [pl.BlockSpec(memory_space=pl.ANY)] * 6,
        out_specs=pl.BlockSpec(memory_space=pltpu.VMEM),
        scratch_shapes=[
            pltpu.VMEM((LOCAL_EXPERTS, width, units), bf16),
            pltpu.VMEM((LOCAL_EXPERTS, width, units), bf16),
            pltpu.VMEM((LOCAL_EXPERTS, units, width), bf16),
            *[pltpu.VMEM(weight.shape, bf16) for weight in shared],
            pltpu.VMEM((n_z, 2, tokens, width), bf16),
            pltpu.VMEM((tp_size, 4, 128), jnp.float32),
            pltpu.VMEM((n_z, LOCAL_EXPERTS, all_slots, width), bf16),
            pltpu.VMEM((n_z, all_slots, width), bf16),
            pltpu.VMEM((all_slots, units), bf16),
            pltpu.VMEM((n_z, all_slots, width), bf16),
            pltpu.VMEM((n_z, all_slots, width), bf16),
            pltpu.VMEM((tokens, width), jnp.float32),
            pltpu.VMEM((tokens, width), jnp.float32),
            pltpu.VMEM((tp_size, 2, 128), jnp.float32),
            pltpu.VMEM((n_z, tokens, width), bf16),
            pltpu.VMEM((n_z, tokens, width), bf16),
            pltpu.VMEM((n_z + 1, tokens, width), bf16),
            pltpu.VMEM((n_z, slots, width) if by_line else (1, 16, 128), bf16),
            pltpu.VMEM((n_z + 1, slots, width) if by_line else (1, 16, 128), bf16),
            pltpu.VMEM((slots, width) if by_line else (8, 128), jnp.float32),
            dma((6,)),
            dma((2, n_z)),
            dma((n_z,)),
            dma((n_z,)),
            dma((n_z,)),
            dma((tp_size,)),
            dma((tp_size,)),
            dma((n_z, n_sp)),
            dma((n_z, n_sp)),
            dma((n_z,)),
            dma((n_z,)),
            dma((n_z,)),
            dma((n_z,)),
            dma((n_z, n_sp)),
            dma((n_z, n_sp)),
            dma((n_z,)),
            dma((n_z,)),
            dma((n_z,)),
            dma((n_z + 1,)),
            dma((2, n_z)),
            dma((n_z,)),
            dma((n_z + 1,)),
        ],
        compiler_params=pltpu.CompilerParams(
            collective_id=1, has_side_effects=True, vmem_limit_bytes=67_000_000
        ),
    )(hidden, meta, *[vec.reshape(1, width) for vec in norm], *shared, expert_gate, expert_up, expert_down)


def local(
    residual,
    wide_query,
    narrow_query,
    wide_keys,
    narrow_keys,
    wide_values,
    narrow_values,
    wide_query_gain,
    wide_key_gain,
    narrow_query_gain,
    narrow_key_gain,
    wide_out,
    narrow_out,
    first_gain,
    first_bias,
    route_ids,
    route_weights,
    expert_gate,
    expert_up,
    expert_down,
    shared_gate,
    shared_up,
    shared_down,
    second_gain,
    second_bias,
):
    hidden = attention(
        (wide_query, narrow_query),
        (wide_keys, narrow_keys, wide_values, narrow_values),
        (wide_query_gain, wide_key_gain, narrow_query_gain, narrow_key_gain),
        residual,
        wide_out,
        narrow_out,
        first_gain,
        first_bias,
    )
    device_rows = hidden.shape[0]
    sp_size = lax.axis_size("sp")
    top_count = route_ids.shape[1]
    experts = LOCAL_EXPERTS * sp_size
    capacity = max(2, (5 * device_rows * top_count + 4 * experts - 1) // (4 * experts))
    meta = jnp.concatenate([route_ids.astype(jnp.float32), route_weights], axis=1)
    meta = jnp.pad(meta, ((0, 128 - device_rows), (0, 0)), constant_values=-1.0).T
    return moe(
        hidden,
        meta,
        (shared_gate, shared_up, shared_down),
        (second_gain, second_bias),
        (expert_gate, expert_up, expert_down),
        capacity,
    )


def solution(mesh):
    in_specs = (
        P(("sp", "tp"), None),
        P("sp", "tp"),
        P("sp", "tp"),
        P("sp", None),
        P("sp", None),
        P("sp", None),
        P("sp", None),
        P(),
        P(),
        P(),
        P(),
        P("tp", None),
        P("tp", None),
        P(),
        P(),
        P(("sp", "tp"), None),
        P(("sp", "tp"), None),
        P("sp", None, "tp"),
        P("sp", None, "tp"),
        P("sp", "tp", None),
        P(),
        P(),
        P(),
        P(),
        P(),
    )
    out_specs = P(("sp", "tp"), None)
    return jax.shard_map(local, mesh=mesh, in_specs=in_specs, out_specs=out_specs, check_vma=False)
```

```python
import functools
import math

import jax
import jax.numpy as jnp
import numpy as np
from jax import lax
from jax.experimental import pallas as pl
from jax.experimental.pallas import tpu as pltpu
from jax.sharding import PartitionSpec as P

WIDE_HEADS = 16
WIDE_GROUPS = 4
NARROW_HEADS = 32
NARROW_GROUPS = 8
GRID_WIDTH = 64
SEQ_SHARDS = 4
LOCAL_EXPERTS = 2


EPS_HEAD = 1e-06
EPS_LAYER = 1e-05
ALPHA = 2.0**0.25
THETA = 10000.0


def greet(tp_size, sp_peers, me_sp, me_tp):
    barrier = pltpu.get_barrier_semaphore()

    @pl.loop(1, tp_size)
    def _(j):
        pl.semaphore_signal(
            barrier,
            inc=1,
            device_id=(me_sp, (me_tp + j) % tp_size),
            device_id_type=pl.DeviceIdType.MESH,
        )

    for sp in sp_peers:
        pl.semaphore_signal(
            barrier, inc=1, device_id=(sp, me_tp), device_id_type=pl.DeviceIdType.MESH
        )
    return lambda: pl.semaphore_wait(barrier, tp_size - 1 + len(sp_peers))


def line_order(place, count, step):
    mirrored = place >= (count + 1) // 2
    near = jnp.where(mirrored, count - 1 - place, place)
    swing = jnp.where(step % 2 == 1, near + (step + 1) // 2, near - step // 2)
    spot = jnp.where(step <= 2 * near, swing, step)
    return jnp.where(mirrored, count - 1 - spot, spot)


def angle_tables(head_size, lanes, grid_rows):
    half, quarter = head_size // 2, head_size // 4
    lane = np.arange(lanes)
    spot = lane % half
    frequency = THETA ** (-(spot % quarter) / quarter)
    by_row = lane % head_size < half
    sign = np.where(spot < quarter, -1.0, 1.0)
    angles = np.arange(max(grid_rows, GRID_WIDTH))[:, None] * frequency[None, :]
    tables = []
    for keep, count in ((by_row, grid_rows), (~by_row, GRID_WIDTH)):
        tables.append(np.where(keep, np.cos(angles[:count]), 0.0))
        tables.append(np.where(keep, sign * np.sin(angles[:count]), 0.0))
    return [table.astype(np.float32) for table in tables]


def attention_kernel(
    wide_query,
    narrow_query,
    wide_keys,
    narrow_keys,
    wide_values,
    narrow_values,
    wide_query_gain,
    wide_key_gain,
    narrow_query_gain,
    narrow_key_gain,
    wide_row_cos,
    wide_row_sin,
    wide_col_cos,
    wide_col_sin,
    narrow_row_cos,
    narrow_row_sin,
    narrow_col_cos,
    narrow_col_sin,
    residual,
    wide_out,
    narrow_out,
    norm_gain,
    norm_bias,
    hidden_ref,
    wide_kv,
    narrow_kv,
    values_ones,
    wide_heads,
    narrow_heads,
    out_all,
    mixed,
    gathered,
    projected,
    load_sem,
    kv_send,
    kv_recv,
    kv_pair_send,
    kv_pair_recv,
    line_send,
    line_recv,
    out_pair_send,
    out_pair_recv,
    share_send,
    share_recv,
    mixed_send,
    mixed_recv,
    *,
    tp_size,
    shards,
    wide_size,
    narrow_size,
    local_wide,
    local_narrow,
):
    n_z = tp_size // 2
    lanes = 128
    tokens, width = residual.shape
    seg_rows = wide_query.shape[0]
    half_rows = seg_rows // 2
    prep_rows = 256
    prep_grid = prep_rows // GRID_WIDTH
    out_rows = wide_out.shape[0]
    piece = 2 * out_rows // shards
    me_sp = lax.axis_index("sp")
    me_tp = lax.axis_index("tp")
    z = me_tp // 2
    core = me_tp % 2
    peer = me_tp + 1 - 2 * core
    shard = me_sp % shards
    first_sp = me_sp - shard
    kinds = (wide_kv, narrow_kv)

    def remote(src, dst, send_sem, recv_sem, sp, tp):
        return pltpu.make_async_remote_copy(
            src_ref=src,
            dst_ref=dst,
            send_sem=send_sem,
            recv_sem=recv_sem,
            device_id=(sp, tp),
            device_id_type=pl.DeviceIdType.MESH,
        )

    def kv_part(kind, owner, side):
        start = pl.multiple_of(owner * seg_rows + side * half_rows, half_rows)
        return kinds[kind].at[pl.ds(start, half_rows)]

    def kv_copy(kind, j):
        part = kv_part(kind, shard, core)
        return remote(
            part, part, kv_send.at[kind, j], kv_recv.at[kind, j], first_sp + (shard + j) % shards, me_tp
        )

    def kv_pair(kind, j):
        part = kv_part(kind, (shard - j + shards) % shards, core)
        return remote(
            part, part, kv_pair_send.at[kind, j], kv_pair_recv.at[kind, j], me_sp, peer
        )

    def out_piece(place, owner):
        start = (2 * place + core) * 2 * out_rows + owner * piece
        return out_all.at[pl.ds(pl.multiple_of(start, piece), piece)]

    def line_copy(place, way):
        part = out_piece(place, shard)
        return remote(
            part, part, line_send.at[way, place], line_recv.at[place], me_sp, me_tp + 2 - 4 * way
        )

    def passes(place, way):
        if way == 0:
            return jnp.logical_and(place <= z, z < n_z - 1)
        return jnp.logical_and(place >= z, z > 0)

    def out_pair(place, j):
        part = out_piece(place, (shard - j + shards) % shards)
        return remote(part, part, out_pair_send.at[place, j], out_pair_recv.at[place, j], me_sp, peer)

    def own_pair():
        part = out_all.at[pl.ds(pl.multiple_of(me_tp * 2 * out_rows, 2 * out_rows), 2 * out_rows)]
        return remote(part, part, out_pair_send.at[z, 0], out_pair_recv.at[z, 0], me_sp, peer)

    def share_copy(place, j):
        part = out_piece(place, shard)
        return remote(
            part, part, share_send.at[place, j], share_recv.at[place, j],
            first_sp + (shard + j) % shards, me_tp,
        )

    def mixed_copy(kind, b):
        target = (me_tp + 1 + b) % tp_size
        return remote(
            mixed.at[kind, target],
            gathered.at[:, pl.ds(pl.multiple_of((2 * me_tp + kind) * lanes, lanes), lanes)],
            mixed_send.at[kind, b],
            mixed_recv.at[kind, b],
            me_sp,
            target,
        )

    loads = [
        pltpu.make_async_copy(
            src,
            out_all.at[pl.ds(pl.multiple_of((2 * me_tp + i) * out_rows, out_rows), out_rows)],
            load_sem.at[i],
        )
        for i, src in enumerate((wide_out, narrow_out))
    ]
    await_peers = greet(
        tp_size, [first_sp + (shard + j) % shards for j in range(1, shards)], me_sp, me_tp
    )
    for copy in loads:
        copy.start()

    lane = lax.broadcasted_iota(jnp.int32, (1, lanes), 1)

    def spread_gain(gain):
        size = gain.shape[1]
        row = lax.broadcasted_iota(jnp.int32, (size, lanes), 0)
        column = lax.broadcasted_iota(jnp.int32, (size, lanes), 1)
        return jnp.dot(
            jnp.broadcast_to(gain[...], (8, size)),
            jnp.where(column % size == row, 1.0, 0.0),
            precision=lax.Precision.HIGHEST,
            preferred_element_type=jnp.float32,
        )[0:1]

    gains = [
        spread_gain(gain)
        for gain in (wide_query_gain, wide_key_gain, narrow_query_gain, narrow_key_gain)
    ]

    def normalized(values, size, gain_row, row_cos, row_sin, col_cos, col_sin, i):
        squares = values * values
        high = squares.astype(jnp.bfloat16)
        low = (squares - high.astype(jnp.float32)).astype(jnp.bfloat16)
        left = lax.broadcasted_iota(jnp.int32, (lanes, lanes), 0) // size
        right = lax.broadcasted_iota(jnp.int32, (lanes, lanes), 1) // size
        same = jnp.where(left == right, 1.0, 0.0).astype(jnp.bfloat16)
        total = jnp.dot(high, same, preferred_element_type=jnp.float32) + jnp.dot(
            low, same, preferred_element_type=jnp.float32
        )
        scaled = values * lax.rsqrt(total * (1.0 / size) + EPS_HEAD) * gains[gain_row]
        quarter = size // 4
        partner = jnp.where(
            lane % (size // 2) < quarter,
            pltpu.roll(scaled, lanes - quarter, 1),
            pltpu.roll(scaled, quarter, 1),
        )
        grid_row = (shard * (seg_rows // prep_rows) + i) * prep_grid

        def spread(by_row, by_col):
            lines = by_row[pl.ds(grid_row, prep_grid), :]
            return jnp.concatenate([lines[g : g + 1, :] + by_col[...] for g in range(prep_grid)], axis=0)

        return scaled * spread(row_cos, col_cos) + partner * spread(row_sin, col_sin)

    wide_tables = (wide_row_cos, wide_row_sin, wide_col_cos, wide_col_sin)
    narrow_tables = (narrow_row_cos, narrow_row_sin, narrow_col_cos, narrow_col_sin)

    def column_pick(source, group, size):
        column = lax.broadcasted_iota(jnp.int32, (source.shape[1], lanes), 0)
        return jnp.where(column == group * size + lane % size, 1.0, 0.0).astype(jnp.bfloat16)

    def key_step(kind, i, keys, values, picks, size, gain_row, tables):
        rows = pl.ds(pl.multiple_of(i * prep_rows, prep_rows), prep_rows)
        own_keys = jnp.dot(keys[rows, :], picks, preferred_element_type=jnp.float32)
        own_values = jnp.dot(values[rows, :], picks, preferred_element_type=jnp.float32)
        rotated = normalized(own_keys, size, gain_row, *tables, i)
        packed = jnp.where((lane // size) % 2 == 0, rotated, own_values).astype(jnp.bfloat16)
        start = pl.multiple_of(shard * seg_rows + i * prep_rows, prep_rows)
        kinds[kind][pl.ds(start, prep_rows), :] = packed

    per_wide = WIDE_HEADS // WIDE_GROUPS
    per_narrow = NARROW_HEADS // NARROW_GROUPS
    wide_picks = column_pick(wide_keys, me_tp * local_wide // per_wide, wide_size)
    lower_group = 2 * z * local_narrow // per_narrow
    upper_group = (2 * z + 1) * local_narrow // per_narrow
    narrow_picks = column_pick(
        narrow_keys, jnp.where(lane < lanes // 2, lower_group, upper_group), narrow_size
    )
    blocks = seg_rows // prep_rows

    @pl.loop(0, blocks)
    def _(i):
        key_step(0, i, wide_keys, wide_values, wide_picks, wide_size, 1, wide_tables)

    await_peers()
    for j in range(1, shards):
        kv_copy(0, j).start()

    for copy in loads:
        copy.wait()
    own_pair().start()

    for way in range(2):

        @pl.when(passes(z, way))
        def _():
            line_copy(z, way).start()

    @pl.loop(0, blocks)
    def _(i):
        key_step(1, i, narrow_keys, narrow_values, narrow_picks, narrow_size, 3, narrow_tables)

    for j in range(1, shards):
        kv_copy(1, j).start()
    @pl.loop(0, blocks)
    def _(i):
        rows = pl.ds(pl.multiple_of(i * prep_rows, prep_rows), prep_rows)
        rotated = normalized(
            wide_query[rows, :].astype(jnp.float32), wide_size, 0, *wide_tables, i
        )
        for h in range(local_wide):
            moved = rotated if h == 0 else pltpu.roll(rotated, lanes - h * wide_size, 1)
            wide_heads[h, rows] = jnp.where(lane < wide_size, moved, 0.0).astype(jnp.bfloat16)
        rotated = normalized(
            narrow_query[rows, :].astype(jnp.float32), narrow_size, 2, *narrow_tables, i
        )
        for h in range(local_narrow):
            shift = (core * (lanes // 2) + lanes - h * narrow_size) % lanes
            moved = pltpu.roll(rotated, shift, 1)
            kept = lane // narrow_size == 2 * core
            narrow_heads[h, rows] = jnp.where(kept, moved, 0.0).astype(jnp.bfloat16)

    def attend(block, kv, size):
        scores = lax.dot_general(
            block, kv[...], (((1,), (1,)), ((), ())), preferred_element_type=jnp.float32
        )
        largest = jnp.max(scores, axis=-1, keepdims=True)
        factor = math.log2(math.e) * size ** (-0.5)
        weights = jnp.exp2((scores - largest) * factor).astype(jnp.bfloat16)
        sums = jnp.dot(weights, values_ones[...], preferred_element_type=jnp.float32)
        return sums / sums[:, 0:1]

    def forward_kv(kind):
        for j in range(1, shards):
            kv_copy(kind, j).wait_recv()
            kv_pair(kind, j).start()

    def arrived_kv(kind):
        for j in range(1, shards):
            kv_pair(kind, j).wait_recv()
        size = (wide_size, narrow_size)[kind]
        keep = jnp.where((lane // size) % 2 == 1, 1.0, 0.0).astype(jnp.bfloat16)
        fill = jnp.where((lane // size) % 2 == 1, 0.0, 1.0).astype(jnp.bfloat16)

        @pl.loop(0, shards * blocks)
        def _(i):
            rows = pl.ds(pl.multiple_of(i * prep_rows, prep_rows), prep_rows)
            values_ones[rows, :] = kinds[kind][rows, :] * keep + fill

    def put_mixed(kind, b, target, value):
        @pl.when(b < tp_size - 1)
        def _():
            mixed[kind, target] = value
            mixed_copy(kind, b).start()

        @pl.when(b == tp_size - 1)
        def _():
            spot = pl.multiple_of((2 * target + kind) * lanes, lanes)
            gathered[:, pl.ds(spot, lanes)] = value

    def line_wait(place):
        part = out_piece(place, shard)
        pltpu.make_async_copy(part, part, line_recv.at[place]).wait()

    def forward_step(step):
        place = line_order(z, n_z, step)
        for way in range(2):

            @pl.when(passes(place, way))
            def _():
                line_wait(place)
                line_copy(place, way).start()

    def share_step(step):
        place = line_order(z, n_z, step)

        @pl.when(jnp.logical_not(jnp.logical_or(passes(place, 0), passes(place, 1))))
        def _():
            line_wait(place)

        for j in range(1, shards):
            share_copy(place, j).start()
        out_pair(place, 0).start()

    forward_kv(0)
    arrived_kv(0)
    for step in range(1, min(3, n_z)):
        forward_step(step)

    @pl.loop(0, tp_size)
    def _(b):
        @pl.when(b == n_z - 1)
        def _():
            forward_kv(1)

        @pl.when(jnp.logical_and(b >= n_z, b < 2 * n_z - 3))
        def _():
            forward_step(b - n_z + 3)

        @pl.when(jnp.logical_or(b == n_z // 2, b == n_z + n_z // 2))
        def _():
            share_step(b // n_z + 1)

        target = (me_tp + 1 + b) % tp_size
        rows = pl.ds(pl.multiple_of(target * tokens, tokens), tokens)
        block = jnp.concatenate([wide_heads[h, rows] for h in range(local_wide)], axis=0)
        values = attend(block, wide_kv, wide_size)
        total = jnp.zeros((tokens, lanes), jnp.float32)
        for h in range(local_wide):
            part = values[h * tokens : (h + 1) * tokens]
            shift = ((h + 1) * wide_size) % lanes
            moved = part if shift == 0 else pltpu.roll(part, shift, 1)
            total = total + jnp.where(lane // wide_size == h, moved, 0.0)
        put_mixed(0, b, target, total.astype(jnp.bfloat16))

    arrived_kv(1)

    @pl.loop(0, tp_size)
    def _(b):
        @pl.when(jnp.logical_and(b > 0, b + 2 < n_z))
        def _():
            share_step(b + 2)

        @pl.when(b > tp_size - n_z)
        def _():
            place = line_order(z, n_z, b - (tp_size - n_z))
            for j in range(1, shards):
                share_copy(place, j).wait_recv()
                out_pair(place, j).start()

        target = (me_tp + 1 + b) % tp_size
        rows = pl.ds(pl.multiple_of(target * tokens, tokens), tokens)
        total = jnp.zeros((tokens, lanes), jnp.float32)
        for first in range(0, local_narrow, 2):
            block = jnp.concatenate([narrow_heads[first + h, rows] for h in range(2)], axis=0)
            values = attend(block, narrow_kv, narrow_size)
            for h in range(2):
                part = values[h * tokens : (h + 1) * tokens]
                shift = (
                    (first + h) * narrow_size + 2 * lanes - core * (lanes // 2) - narrow_size
                ) % lanes
                moved = pltpu.roll(part, shift, 1)
                total = total + jnp.where(lane // narrow_size == first + h, moved, 0.0)
        put_mixed(1, b, target, total.astype(jnp.bfloat16))

    @pl.loop(0, n_z)
    def _(place):
        @pl.when(place == z)
        def _():
            own_pair().wait_recv()

        @pl.when(place != z)
        def _():
            for j in range(shards):
                out_pair(place, j).wait_recv()

    @pl.loop(0, tp_size - 1)
    def _(b):
        mixed_copy(0, b).wait_recv()
        mixed_copy(1, b).wait_recv()

    chunk = 512
    for start in range(0, width, chunk):

        total = ALPHA * residual[:, start : start + chunk].astype(jnp.float32)
        if out_rows == lanes:
            total = total + jnp.dot(
                gathered[...], out_all[:, start : start + chunk], preferred_element_type=jnp.float32
            )
        else:
            for q in range(2 * tp_size):
                total = total + jnp.dot(
                    gathered[:, q * lanes : q * lanes + out_rows],
                    out_all[q * out_rows : (q + 1) * out_rows, start : start + chunk],
                    preferred_element_type=jnp.float32,
                )
        projected[:, start : start + chunk] = total

    values = projected[...]
    center = jnp.mean(values, axis=-1, keepdims=True)
    shifted = values - center
    variance = jnp.mean(shifted * shifted, axis=-1, keepdims=True)
    hidden_ref[...] = (
        shifted * lax.rsqrt(variance + EPS_LAYER) * norm_gain[...] + norm_bias[...]
    ).astype(jnp.bfloat16)

    own_pair().wait_send()
    for j in range(1, shards):
        for kind in range(2):
            kv_copy(kind, j).wait_send()
            kv_pair(kind, j).wait_send()

    @pl.loop(0, n_z)
    def _(place):
        for way in range(2):

            @pl.when(passes(place, way))
            def _():
                line_copy(place, way).wait_send()

        @pl.when(place != z)
        def _():
            for j in range(shards):
                out_pair(place, j).wait_send()
            for j in range(1, shards):
                share_copy(place, j).wait_send()

    @pl.loop(0, tp_size - 1)
    def _(b):
        mixed_copy(0, b).wait_send()
        mixed_copy(1, b).wait_send()


def attention(
    queries, keys_values, gain_vecs, residual, wide_out, narrow_out, first_gain, first_bias
):
    tp_size = lax.axis_size("tp")
    n_z = tp_size // 2
    lanes = 128
    tokens, width = residual.shape
    seg_rows = queries[0].shape[0]
    shards = SEQ_SHARDS
    sizes = gain_vecs[0].shape[0], gain_vecs[2].shape[0]
    local_heads = [q.shape[1] // size for q, size in zip(queries, sizes)]
    queries = [jnp.pad(q, ((0, 0), (0, lanes - q.shape[1]))) for q in queries]
    gains = [gain.reshape(1, -1) for gain in gain_vecs]
    grid_rows = shards * seg_rows // GRID_WIDTH
    tables = [
        jnp.asarray(table)
        for size in sizes
        for table in angle_tables(size, lanes, grid_rows)
    ]
    bf16 = jnp.bfloat16
    dma = pltpu.SemaphoreType.DMA
    vmem = pl.BlockSpec(memory_space=pltpu.VMEM)
    hbm = pl.BlockSpec(memory_space=pl.ANY)
    return pl.pallas_call(
        functools.partial(
            attention_kernel,
            tp_size=tp_size,
            shards=shards,
            wide_size=sizes[0],
            narrow_size=sizes[1],
            local_wide=local_heads[0],
            local_narrow=local_heads[1],
        ),
        out_shape=jax.ShapeDtypeStruct((tokens, width), bf16),
        in_specs=[vmem] * 19 + [hbm] * 2 + [vmem] * 2,
        out_specs=vmem,
        scratch_shapes=[
            pltpu.VMEM((shards * seg_rows, lanes), bf16),
            pltpu.VMEM((shards * seg_rows, lanes), bf16),
            pltpu.VMEM((shards * seg_rows, lanes), bf16),
            pltpu.VMEM((local_heads[0], seg_rows, lanes), bf16),
            pltpu.VMEM((local_heads[1], seg_rows, lanes), bf16),
            pltpu.VMEM((2 * tp_size * wide_out.shape[0], width), bf16),
            pltpu.VMEM((2, tp_size, tokens, lanes), bf16),
            pltpu.VMEM((tokens, 2 * tp_size * lanes), bf16),
            pltpu.VMEM((tokens, width), jnp.float32),
            dma((2,)),
            dma((2, shards)),
            dma((2, shards)),
            dma((2, shards)),
            dma((2, shards)),
            dma((2, n_z)),
            dma((n_z,)),
            dma((n_z, shards)),
            dma((n_z, shards)),
            dma((n_z, shards)),
            dma((n_z, shards)),
            dma((2, tp_size)),
            dma((2, tp_size)),
        ],
        compiler_params=pltpu.CompilerParams(
            collective_id=0, has_side_effects=True, vmem_limit_bytes=66_000_000
        ),
    )(
        *queries,
        *keys_values,
        *gains,
        *tables,
        residual,
        wide_out,
        narrow_out,
        first_gain.reshape(1, width),
        first_bias.reshape(1, width),
    )


def moe_kernel(
    hidden_ref,
    meta_ref,
    norm_gain,
    norm_bias,
    shared_gate_hbm,
    shared_up_hbm,
    shared_down_hbm,
    gate_hbm,
    up_hbm,
    down_hbm,
    out_ref,
    gate_ref,
    up_ref,
    down_ref,
    shared_gate,
    shared_up,
    shared_down,
    hid,
    meta_all,
    rows,
    stage,
    act,
    peer_part,
    ret,
    own_half,
    result,
    spots_all,
    cross_send,
    cross,
    line_in,
    far_in,
    far_line_in,
    far_sum,
    weight_sem,
    z_send,
    z_recv,
    pair_send,
    pair_recv,
    meta_send,
    meta_recv,
    x_send,
    x_recv,
    rows_send,
    rows_recv,
    part_send,
    part_recv,
    ret_send,
    ret_recv,
    cross_send_sem,
    cross_recv,
    line_send,
    line_recv,
    far_send_sem,
    far_line_send,
    far_line_recv,
    *,
    n_sp,
    tp_size,
    cap,
    slots,
    by_line,
):
    n_z = tp_size // 2
    tokens, width = hidden_ref.shape
    all_slots = n_sp * slots
    chunk = 512
    lag = 2
    parts = 4
    cuts = 2
    expert_lines = (LOCAL_EXPERTS * n_sp + 15) // 16 * 16
    me_sp = lax.axis_index("sp")
    me_tp = lax.axis_index("tp")
    z = me_tp // 2
    core = me_tp % 2
    peer = me_tp + 1 - 2 * core
    far_sp = n_sp - 1 - me_sp
    far_send = (2 * n_sp - 1 - 2 * me_sp) % n_sp
    far_recv = (2 * me_sp + 1) % n_sp
    relays = core == 1 if by_line else False

    def skipped(j, far_j, place):
        if not by_line:
            return j < 0
        return jnp.logical_and(core == 1, jnp.logical_and(j == far_j, place != z))

    def is_far(j, far_j):
        if not by_line:
            return j < 0
        return jnp.logical_and(core == 1, j == far_j)

    def remote(src, dst, send_sem, recv_sem, sp, tp):
        return pltpu.make_async_remote_copy(
            src_ref=src,
            dst_ref=dst,
            send_sem=send_sem,
            recv_sem=recv_sem,
            device_id=(sp, tp),
            device_id_type=pl.DeviceIdType.MESH,
        )

    weight_copies = [
        pltpu.make_async_copy(src, dst, weight_sem.at[i])
        for i, (src, dst) in enumerate(
            (
                (shared_gate_hbm, shared_gate),
                (shared_up_hbm, shared_up),
                (shared_down_hbm, shared_down),
                (gate_hbm, gate_ref),
                (up_hbm, up_ref),
                (down_hbm, down_ref),
            )
        )
    ]

    def line_copy(src, way, place, h):
        lines = pl.ds(h * (tokens // cuts), tokens // cuts)
        return remote(
            src.at[lines],
            hid.at[place, core, lines],
            z_send.at[cuts * way + h, place],
            z_recv.at[h, place],
            me_sp,
            me_tp + 2 - 4 * way,
        )

    def pair_copy(src, place):
        return remote(
            src, hid.at[place, core], pair_send.at[place], pair_recv.at[place], me_sp, peer
        )

    def meta_copy(j):
        return remote(
            meta_ref,
            meta_all.at[me_tp],
            meta_send.at[j],
            meta_recv.at[j],
            me_sp,
            (me_tp + j) % tp_size,
        )

    def slot_rows(sp):
        return pl.ds(pl.multiple_of(sp * slots, slots), slots)

    def x_copy(place, j):
        sp = (me_sp + j) % n_sp
        return remote(
            stage.at[place, slot_rows(sp)],
            rows.at[place, core, slot_rows(me_sp)],
            x_send.at[place, j],
            x_recv.at[place, j],
            sp,
            me_tp,
        )

    def far_copy(place):
        return remote(
            stage.at[place, slot_rows(far_sp)],
            far_in.at[place],
            x_send.at[place, far_send],
            x_recv.at[place, far_send],
            far_sp,
            me_tp,
        )

    def far_relay(place, way):
        return remote(
            far_in.at[place],
            far_in.at[place],
            far_send_sem.at[way, place],
            x_recv.at[place, far_recv],
            me_sp,
            me_tp + 2 - 4 * way,
        )

    def far_line(place, way):
        spot = place if way == 0 else jnp.where(place == z - 1, n_z, place)
        return remote(
            rows.at[place, core, slot_rows(far_sp)],
            far_line_in.at[spot],
            far_line_send.at[place],
            far_line_recv.at[spot],
            me_sp,
            me_tp + 2 - 4 * way,
        )

    def passes(place, way):
        if way == 0:
            return jnp.logical_and(place <= z, z < n_z - 1)
        return jnp.logical_and(place >= z, z > 0)

    def rows_copy(place):
        return remote(
            rows.at[place, core],
            rows.at[place, core],
            rows_send.at[place],
            rows_recv.at[place],
            me_sp,
            peer,
        )

    def part_copy(place):
        return remote(
            rows.at[place, 1 - core],
            peer_part.at[place],
            part_send.at[place],
            part_recv.at[place],
            me_sp,
            peer,
        )

    def ret_copy(place, j):
        sp = (me_sp + j) % n_sp
        return remote(
            rows.at[place, core, slot_rows(sp)],
            ret.at[place, slot_rows(me_sp)],
            ret_send.at[place, j],
            ret_recv.at[place, j],
            sp,
            me_tp,
        )

    half_width = width // parts

    def columns(h):
        return pl.ds(h * half_width, half_width)

    def cross_copy(place, h):
        return remote(
            cross_send.at[place, :, columns(h)],
            cross.at[place, :, columns(h)],
            cross_send_sem.at[h, place],
            cross_recv.at[h, place],
            me_sp,
            peer,
        )

    def sum_copy(place, way, h):
        spot = place if way == 0 else jnp.where(place == z - 1, n_z, place)
        return remote(
            cross.at[place, :, columns(h)],
            line_in.at[spot, :, columns(h)],
            line_send.at[h, place],
            line_recv.at[h, spot],
            me_sp,
            me_tp + 2 - 4 * way,
        )

    await_peers = greet(
        tp_size, [(me_sp + j) % n_sp for j in range(1, n_sp)], me_sp, me_tp
    )
    for copy in weight_copies:
        copy.start()
    hid[z, core] = hidden_ref[...]
    meta_all[me_tp] = meta_ref[...]
    await_peers()
    pair_copy(hidden_ref, z).start()

    for h in range(cuts):

        @pl.when(z < n_z - 1)
        def _():
            line_copy(hidden_ref, 0, z, h).start()

        @pl.when(z > 0)
        def _():
            line_copy(hidden_ref, 1, z, h).start()

    @pl.loop(1, tp_size)
    def _(j):
        meta_copy(j).start()

    def selection(place, sp, weighted):
        expert = (LOCAL_EXPERTS * sp + core).astype(jnp.float32)
        parts = []
        for lane in range(2):
            info = meta_all[2 * place + lane]
            line = lax.broadcasted_iota(jnp.int32, (slots, tokens), 0).astype(jnp.float32)
            part = jnp.zeros((slots, tokens), jnp.float32)
            for choice in range(2):
                ids = info[choice : choice + 1, :tokens]
                spots = spots_all[2 * place + lane, choice : choice + 1, :tokens] + lane * cap
                target = jnp.where(ids == expert, spots, -1.0)
                value = info[2 + choice : 3 + choice, :tokens] if weighted else 1.0
                part = part + jnp.where(line == target, value, 0.0)
            parts.append(part)
        return jnp.concatenate(parts, axis=1)

    def clear_far():
        if by_line:

            @pl.when(core == 1)
            def _():
                @pl.loop(0, n_z)
                def _(place):
                    @pl.when(place != z)
                    def _():
                        ret[place, slot_rows(far_sp)] = jnp.zeros((slots, width), jnp.bfloat16)

    def shared_expert():
        for copy in weight_copies[:3]:
            copy.wait()
        gate_values = jnp.dot(hidden_ref[...], shared_gate[...], preferred_element_type=jnp.float32)
        up_values = jnp.dot(hidden_ref[...], shared_up[...], preferred_element_type=jnp.float32)
        active = (jax.nn.silu(gate_values) * up_values).astype(jnp.bfloat16)
        for start in range(0, width, chunk):
            cols = slice(start, start + chunk)
            result[:, cols] = ALPHA * hidden_ref[:, cols].astype(jnp.float32) + jnp.dot(
                active, shared_down[:, cols], preferred_element_type=jnp.float32
            )

    def send_step(step):
        place = line_order(z, n_z, step)

        @pl.when(step > 0)
        def _():
            for h in range(cuts):
                lines = pl.ds(h * (tokens // cuts), tokens // cuts)
                pltpu.make_async_copy(
                    hidden_ref.at[lines], hid.at[place, core, lines], z_recv.at[h, place]
                ).wait()

                @pl.when(jnp.logical_and(place < z, z < n_z - 1))
                def _():
                    line_copy(hid.at[place, core], 0, place, h).start()

                @pl.when(jnp.logical_and(place > z, z > 0))
                def _():
                    line_copy(hid.at[place, core], 1, place, h).start()

            pair_copy(hid.at[place, core], place).start()

        pltpu.make_async_copy(hidden_ref, hid.at[place, 1 - core], pair_recv.at[place]).wait()
        for lane in range(2):
            j = (me_tp - 2 * place - lane + tp_size) % tp_size

            @pl.when(j > 0)
            def _():
                pltpu.make_async_copy(meta_ref, meta_all.at[2 * place + lane], meta_recv.at[j]).wait()

            info = meta_all[2 * place + lane]
            line = lax.broadcasted_iota(jnp.int32, (expert_lines, 128), 0).astype(jnp.float32)
            first = jnp.where(line == info[0:1, :], 1.0, 0.0)
            second = jnp.where(line == info[1:2, :], 1.0, 0.0)
            before = lax.broadcasted_iota(jnp.int32, (128, 128), 0) < lax.broadcasted_iota(
                jnp.int32, (128, 128), 1
            )
            counts = jnp.dot(
                (first + second).astype(jnp.bfloat16),
                jnp.where(before, 1.0, 0.0).astype(jnp.bfloat16),
                preferred_element_type=jnp.float32,
            )
            spots_all[2 * place + lane, 0:1] = jnp.sum(first * counts, axis=0, keepdims=True)
            spots_all[2 * place + lane, 1:2] = jnp.sum(second * counts, axis=0, keepdims=True)

        @pl.loop(0, n_sp)
        def _(i):
            j = (i + 1) % n_sp
            sp = (me_sp + j) % n_sp

            @pl.when(jnp.logical_not(skipped(j, far_send, place)))
            def _():
                picks = selection(place, sp, False).astype(jnp.bfloat16)
                for start in range(0, width, chunk):
                    piece = (
                        jnp.dot(
                            picks[:, :tokens],
                            hid[place, 0, :, start : start + chunk],
                            preferred_element_type=jnp.float32,
                        )
                        + jnp.dot(
                            picks[:, tokens:],
                            hid[place, 1, :, start : start + chunk],
                            preferred_element_type=jnp.float32,
                        )
                    ).astype(jnp.bfloat16)
                    stage[place, slot_rows(sp), start : start + chunk] = piece

                @pl.when(jnp.logical_and(j > 0, jnp.logical_not(is_far(j, far_send))))
                def _():
                    x_copy(place, j).start()

                if by_line:

                    @pl.when(is_far(j, far_send))
                    def _():
                        far_copy(place).start()

            @pl.when(j == 0)
            def _():
                rows[place, core, slot_rows(me_sp)] = stage[place, slot_rows(me_sp)]

    def compute_step(step):
        place = line_order(z, n_z, step)

        if by_line:

            def start_relay(place):
                for way in range(2):

                    @pl.when(passes(place, way))
                    def _():
                        far_relay(place, way).start()

            @pl.when(relays)
            def _():
                @pl.when(step == n_z - 1 - lag)
                def _():
                    for earlier in range(n_z - 1 - lag):
                        start_relay(line_order(z, n_z, earlier))

                far_relay(place, 0).wait_recv()

                @pl.when(step >= n_z - 1 - lag)
                def _():
                    start_relay(place)

                rows[place, core, slot_rows(far_sp)] = far_in[place]

        @pl.loop(1, n_sp)
        def _(j):
            @pl.when(jnp.logical_not(is_far(j, far_recv)))
            def _():
                x_copy(place, j).wait_recv()

        rows_copy(place).start()

        def expert(e):
            block = rows[place, e]
            gate_values = jnp.dot(block, gate_ref[e], preferred_element_type=jnp.float32)
            up_values = jnp.dot(block, up_ref[e], preferred_element_type=jnp.float32)
            act[...] = (jax.nn.silu(gate_values) * up_values).astype(jnp.bfloat16)

        def finish(e):
            for start in range(0, width, chunk):
                rows[place, e, :, start : start + chunk] = jnp.dot(
                    act[...], down_ref[e, :, start : start + chunk], preferred_element_type=jnp.float32
                ).astype(jnp.bfloat16)

        expert(core)
        rows_copy(place).wait_send()
        finish(core)
        rows_copy(place).wait_recv()
        expert(1 - core)
        finish(1 - core)
        part_copy(place).start()

    @pl.loop(0, n_z + lag)
    def _(step):
        @pl.when(step < n_z)
        def _():
            send_step(step)

        @pl.when(step == 0)
        def _():
            if by_line:
                clear_far()
            shared_expert()

        @pl.when(step == lag)
        def _():
            for copy in weight_copies[3:]:
                copy.wait()

        @pl.when(step >= lag)
        def _():
            compute_step(step - lag)

    def return_step(step):
        place = line_order(z, n_z, n_z - 1 - step)
        part_copy(place).wait_recv()

        @pl.loop(0, n_sp)
        def _(i):
            j = (i + 1) % n_sp
            sp = (me_sp + j) % n_sp

            @pl.when(jnp.logical_not(is_far(j, far_send)))
            def _():
                total = (
                    rows[place, core, slot_rows(sp)].astype(jnp.float32)
                    + peer_part[place, slot_rows(sp)].astype(jnp.float32)
                ).astype(jnp.bfloat16)

                @pl.when(j > 0)
                def _():
                    rows[place, core, slot_rows(sp)] = total
                    ret_copy(place, j).start()

                @pl.when(j == 0)
                def _():
                    ret[place, slot_rows(me_sp)] = total

    def far_step(step):
        place = line_order(z, n_z, n_z - 1 - step)

        far_sum[...] = rows[place, core, slot_rows(far_sp)].astype(jnp.float32) + peer_part[
            place, slot_rows(far_sp)
        ].astype(jnp.float32)

        @pl.when(jnp.logical_and(z > 0, place >= z))
        def _():
            pltpu.make_async_copy(
                far_in.at[place], far_line_in.at[place], far_line_recv.at[place]
            ).wait()
            far_sum[...] = far_sum[...] + far_line_in[place].astype(jnp.float32)

        @pl.when(jnp.logical_and(z < n_z - 1, place <= z))
        def _():
            spot = jnp.where(place == z, n_z, place)
            pltpu.make_async_copy(
                far_in.at[place], far_line_in.at[spot], far_line_recv.at[spot]
            ).wait()
            far_sum[...] = far_sum[...] + far_line_in[spot].astype(jnp.float32)

        rows[place, core, slot_rows(far_sp)] = far_sum[...].astype(jnp.bfloat16)

        @pl.when(place == z)
        def _():
            ret_copy(place, far_send).start()

        @pl.when(place > z)
        def _():
            far_line(place, 0).start()

        @pl.when(place < z)
        def _():
            far_line(place, 1).start()

    def combine_step(step):
        place = line_order(z, n_z, n_z - 1 - step)

        @pl.loop(1, n_sp)
        def _(j):
            @pl.when(jnp.logical_not(skipped(j, far_recv, place)))
            def _():
                ret_copy(place, j).wait_recv()

        splits = []
        for lane in range(2):
            info = meta_all[2 * place + lane]
            lines = lax.broadcasted_iota(jnp.int32, (all_slots, tokens), 0).astype(jnp.float32)
            picks = jnp.zeros((all_slots, tokens), jnp.float32)
            for choice in range(2):
                ids = info[choice : choice + 1, :tokens]
                spots = spots_all[2 * place + lane, choice : choice + 1, :tokens] + lane * cap
                shard = jnp.floor(ids * 0.5)
                target = jnp.where(
                    ids - 2.0 * shard == core.astype(jnp.float32), shard * slots + spots, -1.0
                )
                picks = picks + jnp.where(
                    lines == target, info[2 + choice : 3 + choice, :tokens], 0.0
                )
            high = picks.astype(jnp.bfloat16)
            splits.append((high, (picks - high.astype(jnp.float32)).astype(jnp.bfloat16)))

        for h in range(parts):
            for lane in range(2):
                for start in range(h * half_width, (h + 1) * half_width, chunk):
                    piece = sum(
                        lax.dot_general(
                            part,
                            ret[place, :, start : start + chunk],
                            (((0,), (0,)), ((), ())),
                            preferred_element_type=jnp.float32,
                        )
                        for part in splits[lane]
                    )

                    @pl.when(core == lane)
                    def _():
                        own_half[:, start : start + chunk] = piece

                    @pl.when(core != lane)
                    def _():
                        cross_send[place, :, start : start + chunk] = piece.astype(jnp.bfloat16)

            cross_copy(place, h).start()

        for h in range(parts):
            cols = columns(h)
            cross_copy(place, h).wait_recv()
            own_half[:, cols] = own_half[:, cols] + cross[place, :, cols].astype(jnp.float32)

            def add_line(spot):
                pltpu.make_async_copy(
                    cross.at[place, :, cols], line_in.at[spot, :, cols], line_recv.at[h, spot]
                ).wait()
                own_half[:, cols] = own_half[:, cols] + line_in[spot, :, cols].astype(jnp.float32)

            @pl.when(jnp.logical_and(z > 0, place >= z))
            def _():
                add_line(place)

            @pl.when(jnp.logical_and(z < n_z - 1, place <= z))
            def _():
                add_line(jnp.where(place == z, n_z, place))

            @pl.when(place > z)
            def _():
                cross[place, :, cols] = own_half[:, cols].astype(jnp.bfloat16)
                sum_copy(place, 0, h).start()

            @pl.when(place < z)
            def _():
                cross[place, :, cols] = own_half[:, cols].astype(jnp.bfloat16)
                sum_copy(place, 1, h).start()

        @pl.when(place == z)
        def _():
            values = own_half[...] + result[...]
            center = jnp.mean(values, axis=-1, keepdims=True)
            shifted = values - center
            variance = jnp.mean(shifted * shifted, axis=-1, keepdims=True)
            out_ref[...] = (
                shifted * lax.rsqrt(variance + EPS_LAYER) * norm_gain[...] + norm_bias[...]
            ).astype(jnp.bfloat16)

    @pl.loop(0, n_z)
    def _(step):
        return_step(step)

    @pl.loop(0, n_z + 1)
    def _(step):
        if by_line:

            @pl.when(jnp.logical_and(relays, step < n_z))
            def _():
                far_step(step)

        @pl.when(step > 0)
        def _():
            combine_step(step - 1)

    @pl.loop(0, n_z)
    def _(place):
        pair_copy(hidden_ref, place).wait_send()

        @pl.when(jnp.logical_and(place <= z, z < n_z - 1))
        def _():
            for h in range(cuts):
                line_copy(hidden_ref, 0, place, h).wait_send()

        @pl.when(jnp.logical_and(place >= z, z > 0))
        def _():
            for h in range(cuts):
                line_copy(hidden_ref, 1, place, h).wait_send()

        part_copy(place).wait_send()
        for h in range(parts):
            cross_copy(place, h).wait_send()

            @pl.when(place != z)
            def _():
                sum_copy(place, 0, h).wait_send()

        @pl.loop(1, n_sp)
        def _(j):
            @pl.when(jnp.logical_not(skipped(j, far_send, place)))
            def _():
                x_copy(place, j).wait_send()
                ret_copy(place, j).wait_send()

        if by_line:

            @pl.when(relays)
            def _():
                for way in range(2):

                    @pl.when(passes(place, way))
                    def _():
                        far_relay(place, way).wait_send()

                @pl.when(place != z)
                def _():
                    far_line(place, 0).wait_send()

    @pl.loop(1, tp_size)
    def _(j):
        meta_copy(j).wait_send()


def moe(hidden, meta, shared, norm, experts, cap):
    expert_gate, expert_up, expert_down = experts
    n_sp = lax.axis_size("sp")
    tp_size = lax.axis_size("tp")
    n_z = tp_size // 2
    tokens, width = hidden.shape
    units = expert_gate.shape[2]
    slots = (2 * cap + 15) // 16 * 16
    all_slots = n_sp * slots
    by_line = n_sp == 4
    dma = pltpu.SemaphoreType.DMA
    bf16 = jnp.bfloat16
    parts = 4
    cuts = 2
    return pl.pallas_call(
        functools.partial(
            moe_kernel, n_sp=n_sp, tp_size=tp_size, cap=cap, slots=slots, by_line=by_line
        ),
        out_shape=jax.ShapeDtypeStruct((tokens, width), bf16),
        in_specs=[pl.BlockSpec(memory_space=pltpu.VMEM)] * 4
        + [pl.BlockSpec(memory_space=pl.ANY)] * 6,
        out_specs=pl.BlockSpec(memory_space=pltpu.VMEM),
        scratch_shapes=[
            pltpu.VMEM((LOCAL_EXPERTS, width, units), bf16),
            pltpu.VMEM((LOCAL_EXPERTS, width, units), bf16),
            pltpu.VMEM((LOCAL_EXPERTS, units, width), bf16),
            *[pltpu.VMEM(weight.shape, bf16) for weight in shared],
            pltpu.VMEM((n_z, 2, tokens, width), bf16),
            pltpu.VMEM((tp_size, 4, 128), jnp.float32),
            pltpu.VMEM((n_z, LOCAL_EXPERTS, all_slots, width), bf16),
            pltpu.VMEM((n_z, all_slots, width), bf16),
            pltpu.VMEM((all_slots, units), bf16),
            pltpu.VMEM((n_z, all_slots, width), bf16),
            pltpu.VMEM((n_z, all_slots, width), bf16),
            pltpu.VMEM((tokens, width), jnp.float32),
            pltpu.VMEM((tokens, width), jnp.float32),
            pltpu.VMEM((tp_size, 2, 128), jnp.float32),
            pltpu.VMEM((n_z, tokens, width), bf16),
            pltpu.VMEM((n_z, tokens, width), bf16),
            pltpu.VMEM((n_z + 1, tokens, width), bf16),
            pltpu.VMEM((n_z, slots, width) if by_line else (1, 16, 128), bf16),
            pltpu.VMEM((n_z + 1, slots, width) if by_line else (1, 16, 128), bf16),
            pltpu.VMEM((slots, width) if by_line else (8, 128), jnp.float32),
            dma((6,)),
            dma((2 * cuts, n_z)),
            dma((cuts, n_z)),
            dma((n_z,)),
            dma((n_z,)),
            dma((tp_size,)),
            dma((tp_size,)),
            dma((n_z, n_sp)),
            dma((n_z, n_sp)),
            dma((n_z,)),
            dma((n_z,)),
            dma((n_z,)),
            dma((n_z,)),
            dma((n_z, n_sp)),
            dma((n_z, n_sp)),
            dma((parts, n_z)),
            dma((parts, n_z)),
            dma((parts, n_z)),
            dma((parts, n_z + 1)),
            dma((2, n_z)),
            dma((n_z,)),
            dma((n_z + 1,)),
        ],
        compiler_params=pltpu.CompilerParams(
            collective_id=1, has_side_effects=True, vmem_limit_bytes=67_000_000
        ),
    )(hidden, meta, *[vec.reshape(1, width) for vec in norm], *shared, expert_gate, expert_up, expert_down)


def local(
    residual,
    wide_query,
    narrow_query,
    wide_keys,
    narrow_keys,
    wide_values,
    narrow_values,
    wide_query_gain,
    wide_key_gain,
    narrow_query_gain,
    narrow_key_gain,
    wide_out,
    narrow_out,
    first_gain,
    first_bias,
    route_ids,
    route_weights,
    expert_gate,
    expert_up,
    expert_down,
    shared_gate,
    shared_up,
    shared_down,
    second_gain,
    second_bias,
):
    hidden = attention(
        (wide_query, narrow_query),
        (wide_keys, narrow_keys, wide_values, narrow_values),
        (wide_query_gain, wide_key_gain, narrow_query_gain, narrow_key_gain),
        residual,
        wide_out,
        narrow_out,
        first_gain,
        first_bias,
    )
    device_rows = hidden.shape[0]
    sp_size = lax.axis_size("sp")
    top_count = route_ids.shape[1]
    experts = LOCAL_EXPERTS * sp_size
    capacity = max(2, (5 * device_rows * top_count + 4 * experts - 1) // (4 * experts))
    meta = jnp.concatenate([route_ids.astype(jnp.float32), route_weights], axis=1)
    meta = jnp.pad(meta, ((0, 128 - device_rows), (0, 0)), constant_values=-1.0).T
    return moe(
        hidden,
        meta,
        (shared_gate, shared_up, shared_down),
        (second_gain, second_bias),
        (expert_gate, expert_up, expert_down),
        capacity,
    )


def solution(mesh):
    in_specs = (
        P(("sp", "tp"), None),
        P("sp", "tp"),
        P("sp", "tp"),
        P("sp", None),
        P("sp", None),
        P("sp", None),
        P("sp", None),
        P(),
        P(),
        P(),
        P(),
        P("tp", None),
        P("tp", None),
        P(),
        P(),
        P(("sp", "tp"), None),
        P(("sp", "tp"), None),
        P("sp", None, "tp"),
        P("sp", None, "tp"),
        P("sp", "tp", None),
        P(),
        P(),
        P(),
        P(),
        P(),
    )
    out_specs = P(("sp", "tp"), None)
    return jax.shard_map(local, mesh=mesh, in_specs=in_specs, out_specs=out_specs, check_vma=False)
```
